256 devices in a mesh: kv: 32 (over z, x), tp: 8 (over y, core).
Axes of the slice: x: 4, y: 4, z: 8, core: 2. Of those that a mesh axis runs over, the one named last changes fastest.
Arguments:
- stream: bfloat16 [512, 4096], P(None, ('kv', 'tp')), may hold values from -20 to 20
- ssm_state: float32 [512, 64, 64, 128], P('kv', 'tp'), may hold values from -1.8 to 1.8
- conv_state: bfloat16 [512, 3, 8, 768], P('kv', None, 'tp'), may hold values from -6 to 6
- first_gain: float32 [4096], P(('kv', 'tp')), may hold values from 0.1 to 1.9
- first_gate: bfloat16 [4096, 11264], P('kv', 'tp'), may hold values from -0.09375 to 0.09375
- first_up: bfloat16 [4096, 11264], P('kv', 'tp'), may hold values from -0.09375 to 0.09375
- first_down: bfloat16 [11264, 4096], P('tp', 'kv'), may hold values from -0.0546875 to 0.0546875
- mix_gain: float32 [4096], P(('kv', 'tp')), may hold values from 0.1 to 1.9
- gate_in: bfloat16 [4096, 4096], P('kv', 'tp'), may hold values from -0.09375 to 0.09375
- value_in: bfloat16 [4096, 4096], P('kv', 'tp'), may hold values from -0.09375 to 0.09375
- write_in: bfloat16 [4096, 1024], P('kv', 'tp'), may hold values from -0.09375 to 0.09375
- read_in: bfloat16 [4096, 1024], P('kv', 'tp'), may hold values from -0.09375 to 0.09375
- step_in: bfloat16 [4096, 64], P('kv', 'tp'), may hold values from -0.09375 to 0.09375
- conv_weight: float32 [4, 8, 768], P(None, 'tp'), may hold values from -3 to 3
- step_bias: float32 [64], P('tp'), may hold values from -3 to 0.5
- log_decay_rate: float32 [64], P('tp'), may hold values from -1 to 2.5
- group_gain: float32 [4096], P('tp'), may hold values from 0.1 to 1.9
- out_weight: bfloat16 [4096, 4096], P('tp', 'kv'), may hold values from -0.09375 to 0.09375
- last_norm_gain: float32 [4096], P(('kv', 'tp')), may hold values from 0.1 to 1.9
- second_gate: bfloat16 [4096, 11264], P('kv', 'tp'), may hold values from -0.09375 to 0.09375
- second_up: bfloat16 [4096, 11264], P('kv', 'tp'), may hold values from -0.09375 to 0.09375
- second_down: bfloat16 [11264, 4096], P('tp', 'kv'), may hold values from -0.109375 to 0.109375
Outputs:
- next_stream: bfloat16 [512, 4096], P(None, ('kv', 'tp'))
- ssm_next: float32 [512, 64, 64, 128], P('kv', 'tp')
- conv_next: bfloat16 [512, 3, 8, 768], P('kv', None, 'tp')
The draws below stay inside these ranges and needn't reach their ends.
All inputs are finite; a program needn't handle non-finite values.
Results may differ from the reference program's by a relative error of at most 0.015.
Values may be sent and summed in bfloat16 or wider, within the bound.
A program may use at most 64 MiB of HBM per device.

```python
import jax
import jax.numpy as jnp
from jax import lax

D = 4096
FF = 11264
HEADS = 64
HEAD_DIM = 64
STATE = 128
GROUPS = 8
TAPS = 4
SEQS = 512
GROUP_CH = 768
N_KV = 32
N_TP = 8


def draw_stream(key, part):
    noise_key = jax.random.fold_in(jax.random.fold_in(key, 11), 0)
    shard_width = D // (N_KV * N_TP)
    column = jnp.arange(D, dtype=jnp.int32)
    tp_index = column // shard_width % N_TP
    kv_index = column // (shard_width * N_TP)
    tp_frac = tp_index.astype(jnp.float32) / max(N_TP - 1, 1)
    kv_frac = kv_index.astype(jnp.float32) / max(N_KV - 1, 1)
    column_scale = jnp.exp(jnp.log(0.3) + jnp.log(10.0) * tp_frac + jnp.log(1.3) * kv_frac)[None]
    base = jax.random.truncated_normal(noise_key, -4.0, 4.0, (SEQS, D), jnp.float32)
    return (base * column_scale).astype(jnp.bfloat16)


def level_of(rng, dims, cuts, least, high):
    def one(dim, blocks):
        steps = jax.random.uniform(jax.random.fold_in(jax.random.fold_in(rng, 6), dim), (blocks,), jnp.float32, least / len(cuts), high / len(cuts))
        return jnp.repeat(jnp.exp(steps), dims[dim] // blocks).reshape((-1,) + (1,) * (len(dims) - dim - 1))

    loudness = one(*cuts[0])
    for cut in cuts[1:]:
        loudness = loudness * one(*cut)
    return loudness


def scatter_about(key, dims, scale, limit, pieces=(), held_as=jnp.bfloat16):
    result = scale * jax.random.normal(key, dims, jnp.float32)
    if pieces:
        result = result * level_of(key, dims, pieces, -0.22, 0.18)
    return jnp.clip(result, -limit, limit).astype(held_as)


def setup_inputs(seed: int = 0) -> dict:
    seeds = jax.random.split(jax.random.key(seed), 23)
    stream = draw_stream(jax.random.fold_in(seeds[22], 71), 0)
    ssm_state = scatter_about(seeds[1], (SEQS, HEADS, HEAD_DIM, STATE), 0.3, 1.8, ((0, 32), (1, 8)), jnp.float32)
    conv_state = scatter_about(seeds[2], (SEQS, TAPS - 1, GROUPS, GROUP_CH), 1.0, 6.0, ((0, 32), (2, 8)))
    first_gain = jnp.clip(1.0 + 0.18 * jax.random.normal(seeds[3], (D,), jnp.float32), 0.1, 1.9)
    first_gate = scatter_about(seeds[4], (D, FF), D ** -0.5, 0.09375, ((0, 32), (1, 8)))
    first_up = scatter_about(seeds[5], (D, FF), D ** -0.5, 0.09375, ((0, 32), (1, 8)))
    first_down = scatter_about(seeds[6], (FF, D), FF ** -0.5, 0.0546875, ((0, 8), (1, 32)))
    mix_gain = jnp.clip(1.0 + 0.18 * jax.random.normal(seeds[7], (D,), jnp.float32), 0.1, 1.9)
    gate_in = scatter_about(seeds[8], (D, HEADS * HEAD_DIM), D ** -0.5, 0.09375, ((0, 32), (1, 8)))
    value_in = scatter_about(seeds[9], (D, HEADS * HEAD_DIM), D ** -0.5, 0.09375, ((0, 32), (1, 8)))
    write_in = scatter_about(seeds[10], (D, GROUPS * STATE), D ** -0.5, 0.09375, ((0, 32), (1, 8)))
    read_in = scatter_about(seeds[11], (D, GROUPS * STATE), D ** -0.5, 0.09375, ((0, 32), (1, 8)))
    step_in = scatter_about(seeds[12], (D, HEADS), D ** -0.5, 0.09375, ((0, 32), (1, 8)))
    conv_weight = scatter_about(seeds[13], (TAPS, GROUPS, GROUP_CH), TAPS ** -0.5, 3.0, ((1, 8),), jnp.float32)
    step_bias = jnp.clip(-3.0 + 3.5 * jax.random.uniform(seeds[14], (HEADS,), jnp.float32) ** level_of(seeds[14], (HEADS,), ((0, 8),), -0.2, 0.2), -3.0, 0.5)
    log_decay_rate = jnp.clip(-1.0 + 3.5 * jax.random.uniform(seeds[15], (HEADS,), jnp.float32) ** level_of(seeds[15], (HEADS,), ((0, 8),), -0.2, 0.2), -1.0, 2.5)
    group_gain = jnp.clip(1.0 + 0.18 * jax.random.normal(seeds[16], (HEADS * HEAD_DIM,), jnp.float32), 0.1, 1.9)
    out_weight = scatter_about(seeds[17], (HEADS * HEAD_DIM, D), (HEADS * HEAD_DIM) ** -0.5, 0.09375, ((0, 8), (1, 32)))
    last_norm_gain = jnp.clip(1.0 + 0.18 * jax.random.normal(seeds[18], (D,), jnp.float32), 0.1, 1.9)
    second_gate = scatter_about(seeds[19], (D, FF), D ** -0.5, 0.09375, ((0, 32), (1, 8)))
    second_up = scatter_about(seeds[20], (D, FF), D ** -0.5, 0.09375, ((0, 32), (1, 8)))
    second_down = scatter_about(seeds[21], (FF, D), (FF // 4) ** -0.5, 0.109375, ((0, 8), (1, 32)))
    return dict(stream=stream, ssm_state=ssm_state, conv_state=conv_state, first_gain=first_gain, first_gate=first_gate, first_up=first_up, first_down=first_down, mix_gain=mix_gain, gate_in=gate_in, value_in=value_in, write_in=write_in, read_in=read_in, step_in=step_in, conv_weight=conv_weight, step_bias=step_bias, log_decay_rate=log_decay_rate, group_gain=group_gain, out_weight=out_weight, last_norm_gain=last_norm_gain, second_gate=second_gate, second_up=second_up, second_down=second_down)


norm_epsilon = 1e-06

def norm_rows(stream, gain):
    values = stream.astype(jnp.float32)
    scaled = (values * gain.astype(jnp.float32)[None]).astype(jnp.bfloat16)
    factor = lax.rsqrt(lax.optimization_barrier(jnp.mean(values * values, axis=1, keepdims=True)) + norm_epsilon)
    return (scaled, factor)

def blockwise_down(hidden, weight_matrix):
    batch = hidden.shape[0]
    block_list = hidden.reshape(batch, N_TP, -1).astype(jnp.float32)
    split_pieces = weight_matrix.reshape(N_TP, -1, weight_matrix.shape[1]).astype(jnp.float32)
    value_partial_sum = jnp.einsum('noc,oci->noi', block_list, split_pieces).astype(jnp.bfloat16)
    value_partial_sum = lax.optimization_barrier(value_partial_sum)
    return lax.optimization_barrier(jnp.sum(value_partial_sum.astype(jnp.float32), axis=1))

def channel_mixer(stream, gain, gate_weight, up_weight, down_weight):
    scaled, factor = norm_rows(stream, gain)
    gate = jnp.dot(scaled, gate_weight, preferred_element_type=jnp.float32) * factor
    up_sum = jnp.dot(scaled, up_weight, preferred_element_type=jnp.float32) * factor
    hidden = (jax.nn.silu(gate) * up_sum).astype(jnp.bfloat16)
    branch_output = blockwise_down(hidden, down_weight)
    return (stream.astype(jnp.float32) + 0.5 * branch_output).astype(jnp.bfloat16)

def token_mixer(stream, ssm_state, conv_state, gain, gate_in, value_in, write_in, read_in, step_in, conv_weight, step_bias, log_decay_rate, group_gain, out_weight):
    scaled, factor = norm_rows(stream, gain)

    def project(weight_matrix):
        return (jnp.dot(scaled, weight_matrix, preferred_element_type=jnp.float32) * factor).astype(jnp.bfloat16)
    gate = project(gate_in)
    values = project(value_in)
    writes = project(write_in)
    reads = project(read_in)
    steps = project(step_in)
    batch = stream.shape[0]
    groups = conv_weight.shape[1]
    state_size = write_in.shape[1] // groups
    heads = step_in.shape[1]
    head_size = value_in.shape[1] // heads
    per_group = heads // groups
    width = per_group * head_size
    fresh = jnp.concatenate([values.reshape(batch, groups, width), writes.reshape(batch, groups, state_size), reads.reshape(batch, groups, state_size)], axis=2)
    window = jnp.concatenate([conv_state, fresh[:, None]], axis=1)
    activated = jax.nn.silu(lax.optimization_barrier(jnp.sum(window.astype(jnp.float32) * conv_weight.astype(jnp.float32)[None], axis=1)))
    inputs = activated[:, :, :width].reshape(batch, groups, per_group, head_size)
    write_vec = activated[:, :, width:width + state_size]
    read_vec = activated[:, :, width + state_size:]
    step_size = jax.nn.softplus(steps.astype(jnp.float32) + step_bias[None])
    decay = jnp.exp(-step_size * jnp.exp(log_decay_rate)[None])
    step_size = step_size.reshape(batch, groups, per_group)
    decay = decay.reshape(batch, groups, per_group)
    carried = ssm_state.reshape(batch, groups, per_group, head_size, state_size)
    updated = carried * decay[:, :, :, None, None] + (step_size[:, :, :, None] * inputs)[..., None] * write_vec[:, :, None, None, :]
    readout = jnp.einsum('bghpn,bgn->bghp', updated, read_vec).reshape(batch, groups, width)
    gated = readout * jax.nn.silu(gate.astype(jnp.float32)).reshape(batch, groups, width)
    normed = gated * lax.rsqrt(lax.optimization_barrier(jnp.mean(gated * gated, axis=2, keepdims=True)) + norm_epsilon)
    mixed = (normed * group_gain.reshape(groups, width)[None]).astype(jnp.bfloat16).reshape(batch, groups * width)
    branch_output = blockwise_down(mixed, out_weight)
    after = (stream.astype(jnp.float32) + branch_output).astype(jnp.bfloat16)
    return (after, updated.reshape(ssm_state.shape), window[:, 1:])

def reference(stream, ssm_state, conv_state, first_gain, first_gate, first_up, first_down, mix_gain, gate_in, value_in, write_in, read_in, step_in, conv_weight, step_bias, log_decay_rate, group_gain, out_weight, last_norm_gain, second_gate, second_up, second_down):
    after_first = channel_mixer(stream, first_gain, first_gate, first_up, first_down)
    after_mix, ssm_next, conv_next = token_mixer(after_first, ssm_state, conv_state, mix_gain, gate_in, value_in, write_in, read_in, step_in, conv_weight, step_bias, log_decay_rate, group_gain, out_weight)
    next_stream = channel_mixer(after_mix, last_norm_gain, second_gate, second_up, second_down)
    return (next_stream, ssm_next, conv_next)
```

```python
import jax
import jax.numpy as jnp
from jax import lax
from jax.experimental import pallas as pl
from jax.experimental.pallas import tpu as pltpu
from jax.sharding import PartitionSpec as P

MESH = pl.DeviceIdType.MESH
F32, BF16 = jnp.float32, jnp.bfloat16

NZ, NX, NY, NC = 8, 4, 4, 2
NKV, NTP = NZ * NX, NY * NC
SEQS, D, FF = 512, 4096, 11264
OWN = D // (NKV * NTP)
FEAT = OWN * NTP
DEPTH = FEAT * NZ
CUT = FF // NTP // NZ
XS = SEQS // NX
ROWS = SEQS // NKV
HEAD, STATE, PER = 64, 128, 8
MIX = 176
WIDE = 256
norm_epsilon = 1e-06
Z_ORDER = (4, 3, 5, 2, 6, 1, 7)


class Wire:
    def __init__(self, sends, recvs):
        self.sends, self.recvs, self.count, self.open = sends, recvs, 0, []
        kv, self.tp = lax.axis_index("kv"), lax.axis_index("tp")
        self.kv = kv
        self.z, self.x = lax.div(kv, NX), lax.rem(kv, NX)
        self.y, self.c = lax.div(self.tp, NC), lax.rem(self.tp, NC)

    def send(self, src, dst, kv, tp):
        number = self.count
        self.count += 1
        copy = pltpu.make_async_remote_copy(
            src_ref=src,
            dst_ref=dst,
            send_sem=self.sends.at[number],
            recv_sem=self.recvs.at[number],
            device_id=(kv, tp),
            device_id_type=MESH,
        )
        copy.start()
        self.open.append(copy)
        return number

    def recv(self, number, dst, kv, tp):
        pltpu.make_async_remote_copy(
            src_ref=dst,
            dst_ref=dst,
            send_sem=self.sends.at[number],
            recv_sem=self.recvs.at[number],
            device_id=(kv, tp),
            device_id_type=MESH,
        ).wait_recv()

    def drain(self):
        for copy in self.open:
            copy.wait_send()
        self.open = []

    def along_z(self, d):
        return lax.rem(self.z + d, NZ)

    def along_x(self, d):
        return lax.rem(self.x + d, NX)

    def along_y(self, d):
        return lax.rem(self.y + d, NY)

    def along_tp(self, d):
        return lax.rem(self.tp + d, NTP)

    def to_z(self, src, dst):
        out = {}
        for d in Z_ORDER:
            peer = self.along_z(d)
            out[d] = self.send(src(peer), dst, peer * NX + self.x, self.tp)
        return out

    def from_z(self, numbers, dst):
        for d in reversed(Z_ORDER):
            peer = self.along_z(NZ - d)
            self.recv(numbers[d], dst(peer), peer * NX + self.x, self.tp)

    def to_x(self, src, dst):
        out = {}
        for d in (2, 1, 3):
            peer = self.along_x(d)
            out[d] = self.send(src(peer), dst, self.z * NX + peer, self.tp)
        return out

    def from_x(self, numbers, dst):
        for d in (1, 3, 2):
            peer = self.along_x(NX - d)
            self.recv(numbers[d], dst(peer), self.z * NX + peer, self.tp)

    def to_y(self, src, dst):
        out = {}
        for d in (2, 1, 3):
            peer = self.along_y(d)
            out[d] = self.send(src(peer), dst, self.kv, peer * NC + self.c)
        return out

    def from_y(self, numbers, dst):
        for d in (1, 3, 2):
            peer = self.along_y(NY - d)
            self.recv(numbers[d], dst(peer), self.kv, peer * NC + self.c)

    def to_tp(self, src, dst):
        out = {}
        for d in range(1, NTP):
            peer = self.along_tp(d)
            out[d] = self.send(src(peer), dst, self.kv, peer)
        return out

    def from_tp(self, numbers, dst):
        for d in range(1, NTP):
            peer = self.along_tp(NTP - d)
            self.recv(numbers[d], dst(peer), self.kv, peer)


def greet(wire, all_kv):
    barrier = pltpu.get_barrier_semaphore()

    def tell(kv, tp):
        pl.semaphore_signal(barrier, inc=1, device_id=(kv, tp), device_id_type=MESH)

    if all_kv:

        @pl.loop(1, NKV)
        def _(d):
            tell(lax.rem(wire.kv + d, NKV), wire.tp)

        count = NKV - 1
    else:
        for d in range(1, NZ):
            tell(wire.along_z(d) * NX + wire.x, wire.tp)
        for d in range(1, NX):
            tell(wire.z * NX + wire.along_x(d), wire.tp)
        count = NZ - 1 + NX - 1
    for d in range(1, NTP):
        tell(wire.kv, wire.along_tp(d))
    count += NTP - 1
    return lambda: pl.semaphore_wait(barrier, count)


def at_rows(start, size, step):
    return pl.ds(pl.multiple_of(start * step, step), size)


def turn_columns(src, dst):
    for j in range(src.shape[1] // 128):
        dst[j * 128 : (j + 1) * 128, :] = src[:, j * 128 : (j + 1) * 128].T


def send_gate_up(wire, gate_t, up_t, both):
    z = wire.z
    lanes = at_rows(z, FEAT, FEAT)

    def cut(ref):
        return lambda peer: ref.at[at_rows(peer, CUT, CUT), :]

    first = wire.to_z(cut(gate_t), both.at[0:CUT, lanes])
    second = wire.to_z(cut(up_t), both.at[CUT : 2 * CUT, lanes])
    own = at_rows(z, CUT, CUT)
    both[0:CUT, lanes] = gate_t[own, :]
    both[CUT : 2 * CUT, lanes] = up_t[own, :]
    return first, second


def wait_gate_up(wire, numbers, both):
    wire.from_z(numbers[0], lambda s: both.at[0:CUT, at_rows(s, FEAT, FEAT)])
    wire.from_z(numbers[1], lambda s: both.at[CUT : 2 * CUT, at_rows(s, FEAT, FEAT)])


def send_down(wire, down, parts):
    numbers = wire.to_z(lambda peer: down.at[at_rows(peer, CUT, CUT), :], parts.at[wire.z])
    parts[wire.z] = down[at_rows(wire.z, CUT, CUT), :]
    return numbers


def wait_down(wire, numbers, parts, turned):
    wire.from_z(numbers, lambda s: parts.at[s])
    for s in range(NZ):
        turned[s] = parts[s].T


def gather_features(wire, values, gain, feats, sq_z, sq_tp, after_first_sends):
    z, tp, y, c = wire.z, wire.tp, wire.y, wire.c
    wide = values.astype(F32)
    feats[z, tp] = (wide * gain[...]).astype(BF16)
    sq_z[z] = jnp.sum(wide * wide, axis=0, keepdims=True)
    n_feats = wire.to_z(lambda peer: feats.at[z, tp], feats.at[z, tp])
    n_sq = wire.to_z(lambda peer: sq_z.at[z], sq_z.at[z])
    after_first_sends()
    wire.from_z(n_feats, lambda s: feats.at[s, tp])
    sibling = y * NC + (1 - c)
    mine = feats.at[:, tp]
    n_y = wire.to_y(lambda peer: mine, mine)
    n_own = wire.send(mine, mine, wire.kv, sibling)
    wire.from_z(n_sq, lambda s: sq_z.at[s])
    sq_tp[tp] = jnp.sum(sq_z[...], axis=0)
    n_sq2 = wire.to_tp(lambda peer: sq_tp.at[tp], sq_tp.at[tp])
    passed = {}
    for d in (1, 3, 2):
        peer = wire.along_y(NY - d)
        block = feats.at[:, peer * NC + c]
        wire.recv(n_y[d], block, wire.kv, peer * NC + c)
        passed[d] = wire.send(block, block, wire.kv, sibling)
    wire.from_tp(n_sq2, lambda s: sq_tp.at[s])
    wire.recv(n_own, feats.at[:, sibling], wire.kv, sibling)
    for d in (1, 3, 2):
        peer = wire.along_y(NY - d)
        wire.recv(passed[d], feats.at[:, peer * NC + 1 - c], wire.kv, sibling)
    return jnp.sum(sq_tp[...], axis=0)


def channel_mixer(wire, values, gain, s, after_first_sends, wait_weights, wait_down_weights, down_t):
    x = wire.x
    squares = gather_features(wire, values, gain, s["feats"], s["sq_z"], s["sq_tp"], after_first_sends)
    s["sq_x"][x] = squares
    n_sq = wire.to_x(lambda peer: s["sq_x"].at[x], s["sq_x"].at[x])
    wait_weights()
    sums = s["sums"]
    sums[...] = jnp.dot(
        s["both"][...], s["feats"][...].reshape(DEPTH, SEQS), preferred_element_type=F32
    ).astype(BF16)
    sums_x = s["sums_x"]
    n_sums = wire.to_x(lambda peer: sums.at[:, at_rows(peer, XS, XS)], sums_x.at[x])
    sums_x[x] = sums[:, at_rows(x, XS, XS)]
    wait_down_weights()
    wire.from_x(n_sq, lambda p: s["sq_x"].at[p])
    factor = lax.rsqrt(jnp.sum(s["sq_x"][...], axis=0) / D + norm_epsilon)
    s["factor"][...] = factor
    factor = s["factor"][:, at_rows(x, XS, XS)]
    wire.from_x(n_sums, lambda p: sums_x.at[p])
    gates = sum(sums_x[p, 0:CUT].astype(F32) for p in range(NX)) * factor
    ups = sum(sums_x[p, CUT : 2 * CUT].astype(F32) for p in range(NX)) * factor
    hidden = s["hidden"]
    here = hidden.at[:, at_rows(x, XS, XS)]
    here[...] = (gates / (1.0 + jnp.exp(-gates)) * ups).astype(BF16)
    n_hidden = wire.to_x(lambda peer: here, here)
    wire.from_x(n_hidden, lambda p: hidden.at[:, at_rows(p, XS, XS)])
    outs = s["outs"]

    @pl.loop(0, NZ)
    def _(k):
        part = jnp.dot(down_t[k], hidden[...], preferred_element_type=F32)
        outs[k] = part.astype(BF16).reshape(NY, NC, OWN, SEQS)

    c, y, z = wire.c, wire.y, wire.z
    sibling = y * NC + (1 - c)
    other = s["other"]
    n_core = wire.send(outs.at[:, :, 1 - c], other, wire.kv, sibling)
    wire.recv(n_core, other, wire.kv, sibling)
    by_y, arrived_y = s["by_y"], s["arrived_y"]

    @pl.loop(0, NZ)
    def _(k):
        total = outs[k, :, c].astype(F32) + other[k].astype(F32)
        by_y[:, k] = total.astype(BF16)

    n_y = wire.to_y(lambda peer: by_y.at[peer], arrived_y.at[y])
    arrived_y[y] = by_y[y]
    wire.from_y(n_y, lambda p: arrived_y.at[p])
    by_z, arrived_z = s["by_z"], s["arrived_z"]
    by_z[...] = sum(arrived_y[p].astype(F32) for p in range(NY)).astype(BF16)
    n_z = wire.to_z(lambda peer: by_z.at[peer], arrived_z.at[z])
    arrived_z[z] = by_z[z]
    wire.from_z(n_z, lambda p: arrived_z.at[p])
    return jnp.sum(arrived_z[...].astype(F32), axis=0)


FF_SCRATCH = dict(
    feats=((NZ, NTP, OWN, SEQS), BF16),
    sq_z=((NZ, 1, SEQS), F32),
    sq_tp=((NTP, 1, SEQS), F32),
    sq_x=((NX, 1, SEQS), F32),
    factor=((1, SEQS), F32),
    gate_t=((NZ * CUT, FEAT), BF16),
    up_t=((NZ * CUT, FEAT), BF16),
    both=((2 * CUT, DEPTH), BF16),
    sums=((2 * CUT, SEQS), BF16),
    sums_x=((NX, 2 * CUT, XS), BF16),
    hidden=((CUT, SEQS), BF16),
    outs=((NZ, NY, NC, OWN, SEQS), BF16),
    other=((NZ, NY, OWN, SEQS), BF16),
    by_y=((NY, NZ, OWN, SEQS), BF16),
    arrived_y=((NY, NZ, OWN, SEQS), BF16),
    by_z=((NZ, OWN, SEQS), BF16),
    arrived_z=((NZ, OWN, SEQS), BF16),
)

A_SCRATCH = dict(
    FF_SCRATCH,
    down_parts=((NZ, CUT, FEAT), BF16),
    down_t=((NZ, FEAT, CUT), BF16),
    next_parts=((NZ, CUT, FEAT), BF16),
    mix_t=((NZ, MIX, FEAT), BF16),
    mix_in=((MIX, DEPTH), BF16),
    mix_feats=((NZ, NTP, OWN, SEQS), BF16),
    mix_sq_z=((NZ, 1, SEQS), F32),
    mix_sq_tp=((NTP, 1, SEQS), F32),
    turned=((WIDE, SEQS), F32),
    rows=((NKV, ROWS, WIDE), BF16),
    rows_in=((NKV, ROWS, WIDE), BF16),
)

B_SCRATCH = dict(
    FF_SCRATCH,
    mixed_all=((NZ, NX, ROWS, PER * HEAD), BF16),
    out_t=((NTP, OWN, SEQS), BF16),
    out_in=((NTP, OWN, SEQS), BF16),
)


def before_state(*refs):
    (stream, gain, mix_gain, gate, up, down, gate_in, value_in, write_in, read_in, step_in, next_down) = refs[:12]
    after_first, projected, next_down_t = refs[12:15]
    s = dict(zip(A_SCRATCH, refs[15:]))
    wire = Wire(*refs[15 + len(A_SCRATCH) : 17 + len(A_SCRATCH)])
    row_sends, row_recvs = refs[17 + len(A_SCRATCH) :]
    z, x, kv, tp = wire.z, wire.x, wire.kv, wire.tp
    wait_greeting = greet(wire, True)
    turn_columns(gate, s["gate_t"])
    turn_columns(up, s["up_t"])
    wait_greeting()

    def turn_mixer():
        for j in range(PER * HEAD // 128):
            for ref, at in ((gate_in, 0), (value_in, HEAD)):
                tile = ref[:, j * 128 : (j + 1) * 128].T
                s["mix_t"][2 * j, at : at + HEAD] = tile[:HEAD]
                s["mix_t"][2 * j + 1, at : at + HEAD] = tile[HEAD:]
        for ref, base in ((write_in, 0), (read_in, 4)):
            tile = ref[...].T
            for j in range(4):
                s["mix_t"][base + j, 2 * HEAD : 2 * HEAD + 32] = tile[32 * j : 32 * (j + 1)]
        for j in range(NZ):
            s["mix_t"][j, 2 * HEAD + 32 : MIX] = step_in[...]

    numbers = {}

    def weights_out():
        numbers["both"] = send_gate_up(wire, s["gate_t"], s["up_t"], s["both"])
        numbers["down"] = send_down(wire, down, s["down_parts"])
        turn_mixer()
        lanes = at_rows(z, FEAT, FEAT)
        numbers["mix"] = wire.to_z(lambda peer: s["mix_t"].at[peer], s["mix_in"].at[:, lanes])
        s["mix_in"][:, lanes] = s["mix_t"][z]

    branch = channel_mixer(
        wire,
        stream[...],
        gain,
        s,
        weights_out,
        lambda: wait_gate_up(wire, numbers["both"], s["both"]),
        lambda: wait_down(wire, numbers["down"], s["down_parts"], s["down_t"]),
        s["down_t"],
    )
    after = (stream[...].astype(F32) + 0.5 * branch).astype(BF16)
    after_first[...] = after

    def next_weights():
        numbers["next"] = send_down(wire, next_down, s["next_parts"])

    squares = gather_features(wire, after, mix_gain, s["mix_feats"], s["mix_sq_z"], s["mix_sq_tp"], next_weights)
    wire.from_z(numbers["mix"], lambda p: s["mix_in"].at[:, at_rows(p, FEAT, FEAT)])
    part = jnp.dot(s["mix_in"][...], s["mix_feats"][...].reshape(DEPTH, SEQS), preferred_element_type=F32)
    turned = s["turned"]
    turned[2 * HEAD :, :] = jnp.zeros((WIDE - 2 * HEAD, SEQS), F32)
    turned[: 2 * HEAD, :] = part[: 2 * HEAD]
    quarter = lax.rem(z, 4)
    turned[pl.ds(pl.multiple_of(128 + 32 * quarter, 32), 32), :] = part[2 * HEAD : 2 * HEAD + 32]
    beside = pl.multiple_of(128 + 32 * lax.rem(z + 1, 4), 32)
    turned[pl.ds(beside, 8), :] = part[2 * HEAD + 32 : 2 * HEAD + 40]
    turned[pl.ds(pl.multiple_of(beside + 8, 8), 8), :] = jnp.broadcast_to(squares, (8, SEQS))
    rows, rows_in = s["rows"], s["rows_in"]
    rows[...] = turned[...].T.astype(BF16).reshape(NKV, ROWS, WIDE)

    def row_copy(d, peer, slot):
        return pltpu.make_async_remote_copy(
            src_ref=rows.at[peer],
            dst_ref=rows_in.at[slot],
            send_sem=row_sends.at[d],
            recv_sem=row_recvs.at[d],
            device_id=(peer, tp),
            device_id_type=MESH,
        )

    @pl.loop(1, NKV)
    def _(d):
        row_copy(d, lax.rem(kv + d, NKV), kv).start()

    rows_in[kv] = rows[kv]
    wire.from_z(numbers["next"], lambda p: s["next_parts"].at[p])
    for k in range(NZ):
        next_down_t[k] = s["next_parts"][k].T

    @pl.loop(1, NKV)
    def _(d):
        peer = lax.rem(kv + NKV - d, NKV)
        row_copy(d, peer, peer).wait_recv()

    for k in range(NZ):
        projected[k] = sum(rows_in[k * NX + p].astype(F32) for p in range(NX))

    wire.drain()

    @pl.loop(1, NKV)
    def _(d):
        row_copy(d, lax.rem(kv + d, NKV), kv).wait_send()


def after_state(*refs):
    (after_first, mixed, out_weight, gain, gate, up, down_t) = refs[:7]
    result = refs[7]
    s = dict(zip(B_SCRATCH, refs[8:]))
    wire = Wire(*refs[8 + len(B_SCRATCH) :])
    z, x, kv, tp = wire.z, wire.x, wire.kv, wire.tp
    wait_greeting = greet(wire, False)
    mixed_all = s["mixed_all"]
    mixed_all[z, x] = mixed[...]
    wait_greeting()
    n_z = wire.to_z(lambda peer: mixed_all.at[z, x], mixed_all.at[z, x])
    turn_columns(gate, s["gate_t"])
    turn_columns(up, s["up_t"])
    n_both = send_gate_up(wire, s["gate_t"], s["up_t"], s["both"])
    wire.from_z(n_z, lambda p: mixed_all.at[p, x])
    column = mixed_all.at[:, x]
    n_x = wire.to_x(lambda peer: column, column)
    wire.from_x(n_x, lambda p: mixed_all.at[:, p])
    part = jnp.dot(mixed_all[...].reshape(SEQS, PER * HEAD), out_weight[...], preferred_element_type=F32)
    out_t, out_in = s["out_t"], s["out_in"]
    out_t[...] = part.T.astype(BF16).reshape(NTP, OWN, SEQS)
    n_tp = wire.to_tp(lambda peer: out_t.at[peer], out_in.at[tp])
    out_in[tp] = out_t[tp]
    wire.from_tp(n_tp, lambda p: out_in.at[p])
    after = (after_first[...].astype(F32) + jnp.sum(out_in[...].astype(F32), axis=0)).astype(BF16)
    branch = channel_mixer(
        wire,
        after,
        gain,
        s,
        lambda: None,
        lambda: wait_gate_up(wire, n_both, s["both"]),
        lambda: None,
        down_t,
    )
    result[...] = (after.astype(F32) + 0.5 * branch).astype(BF16)
    wire.drain()


def call(body, name, number, outs, scratch, copies, extra, *args):
    memory = [pltpu.VMEM(shape, dtype) for shape, dtype in scratch.values()]
    memory += [pltpu.SemaphoreType.DMA((copies,))] * 2
    memory += extra
    whole = pl.BlockSpec(memory_space=pltpu.VMEM)
    return pl.pallas_call(
        body,
        name=name,
        out_shape=outs,
        in_specs=[whole] * len(args),
        out_specs=jax.tree.map(lambda _: whole, outs),
        scratch_shapes=memory,
        compiler_params=pltpu.CompilerParams(
            collective_id=number, has_side_effects=True, vmem_limit_bytes=48 * 1024 * 1024
        ),
    )(*args)


def state_update(
    projected, ssm_state, conv_state, conv_weight, step_bias, log_decay_rate, group_gain
):
    total = projected[3, :, 2 * HEAD + 8]
    factor = lax.rsqrt(total / D + norm_epsilon)
    scaled = (projected * factor[None, :, None]).astype(BF16)
    gate = scaled[:, :, :HEAD].transpose(1, 0, 2)
    values = scaled[:, :, HEAD : 2 * HEAD].transpose(1, 0, 2).reshape(ROWS, PER * HEAD)
    tile = scaled[:, :, 2 * HEAD :]
    shared = [tile[k, :, 32 * (k % 4) : 32 * (k % 4) + 32] for k in range(NZ)]
    steps = tile[3, :, :PER]
    fresh = jnp.concatenate([values, *shared], axis=1)
    window = jnp.concatenate([conv_state[:, :, 0], fresh[:, None]], axis=1)
    activated = jax.nn.silu(jnp.sum(window.astype(F32) * conv_weight[None, :, 0], axis=1))
    inputs = activated[:, : PER * HEAD].reshape(ROWS, PER, HEAD)
    write_vec = activated[:, PER * HEAD : PER * HEAD + STATE]
    read_vec = activated[:, PER * HEAD + STATE :]
    step_size = jax.nn.softplus(steps.astype(F32) + step_bias[None])
    decay = jnp.exp(-step_size * jnp.exp(log_decay_rate)[None])
    updated = (
        ssm_state * decay[:, :, None, None]
        + (step_size[:, :, None] * inputs)[..., None] * write_vec[:, None, None, :]
    )
    readout = jnp.einsum("bhpn,bn->bhp", updated, read_vec)
    gated = (readout * jax.nn.silu(gate.astype(F32))).reshape(ROWS, PER * HEAD)
    normed = gated * lax.rsqrt(jnp.mean(gated * gated, axis=1, keepdims=True) + norm_epsilon)
    mixed = (normed * group_gain[None]).astype(BF16)
    return mixed, updated, window[:, 1:, None]


def on_device(
    stream,
    ssm_state,
    conv_state,
    first_gain,
    first_gate,
    first_up,
    first_down,
    mix_gain,
    gate_in,
    value_in,
    write_in,
    read_in,
    step_in,
    conv_weight,
    step_bias,
    log_decay_rate,
    group_gain,
    out_weight,
    last_norm_gain,
    second_gate,
    second_up,
    second_down,
):
    step_t = jnp.pad(step_in.T, ((0, MIX - 2 * HEAD - 32 - PER), (0, 0)))
    after_first, projected, next_down_t = call(
        before_state,
        "before_state",
        0,
        (
            jax.ShapeDtypeStruct((OWN, SEQS), BF16),
            jax.ShapeDtypeStruct((NZ, ROWS, WIDE), F32),
            jax.ShapeDtypeStruct((NZ, FEAT, CUT), BF16),
        ),
        A_SCRATCH,
        140,
        [pltpu.SemaphoreType.DMA((NKV,))] * 2,
        stream.T,
        first_gain[:, None],
        mix_gain[:, None],
        first_gate,
        first_up,
        first_down,
        gate_in,
        value_in,
        write_in,
        read_in,
        step_t,
        second_down,
    )
    mixed, ssm_next, conv_next = state_update(
        projected, ssm_state, conv_state, conv_weight, step_bias, log_decay_rate, group_gain
    )
    result = call(
        after_state,
        "after_state",
        1,
        jax.ShapeDtypeStruct((OWN, SEQS), BF16),
        B_SCRATCH,
        100,
        [],
        after_first,
        mixed,
        out_weight,
        last_norm_gain[:, None],
        second_gate,
        second_up,
        next_down_t,
    )
    return (result.T, ssm_next, conv_next)


def solution(mesh):
    placed = (
        P(None, ("kv", "tp")),
        P("kv", "tp", None, None),
        P("kv", None, "tp", None),
        P(("kv", "tp")),
        P("kv", "tp"),
        P("kv", "tp"),
        P("tp", "kv"),
        P(("kv", "tp")),
        P("kv", "tp"),
        P("kv", "tp"),
        P("kv", "tp"),
        P("kv", "tp"),
        P("kv", "tp"),
        P(None, "tp", None),
        P("tp"),
        P("tp"),
        P("tp"),
        P("tp", "kv"),
        P(("kv", "tp")),
        P("kv", "tp"),
        P("kv", "tp"),
        P("tp", "kv"),
    )
    return jax.shard_map(
        on_device,
        mesh=mesh,
        in_specs=placed,
        out_specs=(P(None, ("kv", "tp")), P("kv", "tp", None, None), P("kv", None, "tp", None)),
        check_vma=False,
    )
```

```python
import jax
import jax.numpy as jnp
from jax import lax
from jax.experimental import pallas as pl
from jax.experimental.pallas import tpu as pltpu
from jax.sharding import PartitionSpec as P

MESH = pl.DeviceIdType.MESH
F32, BF16 = jnp.float32, jnp.bfloat16

NZ, NX, NY, NC = 8, 4, 4, 2
NKV, NTP = NZ * NX, NY * NC
SEQS, D, FF = 512, 4096, 11264
OWN = D // (NKV * NTP)
FEAT = OWN * NTP
DEPTH = FEAT * NZ
CUT = FF // NTP // NZ
XS = SEQS // NX
ROWS = SEQS // NKV
HEAD, STATE, PER = 64, 128, 8
MIX = 176
WIDE = 256
norm_epsilon = 1e-06
Z_ORDER = (4, 3, 5, 2, 6, 1, 7)
Z_NEAR = (1, 7, 2, 6, 3, 5, 4)


class Wire:
    def __init__(self, sends, recvs):
        self.sends, self.recvs, self.count, self.open = sends, recvs, 0, []
        kv, self.tp = lax.axis_index("kv"), lax.axis_index("tp")
        self.kv = kv
        self.z, self.x = lax.div(kv, NX), lax.rem(kv, NX)
        self.y, self.c = lax.div(self.tp, NC), lax.rem(self.tp, NC)

    def send(self, src, dst, kv, tp):
        number = self.count
        self.count += 1
        copy = pltpu.make_async_remote_copy(
            src_ref=src,
            dst_ref=dst,
            send_sem=self.sends.at[number],
            recv_sem=self.recvs.at[number],
            device_id=(kv, tp),
            device_id_type=MESH,
        )
        copy.start()
        self.open.append(copy)
        return number

    def recv(self, number, dst, kv, tp):
        pltpu.make_async_remote_copy(
            src_ref=dst,
            dst_ref=dst,
            send_sem=self.sends.at[number],
            recv_sem=self.recvs.at[number],
            device_id=(kv, tp),
            device_id_type=MESH,
        ).wait_recv()

    def drain(self):
        for copy in self.open:
            copy.wait_send()
        self.open = []

    def along_z(self, d):
        return lax.rem(self.z + d, NZ)

    def along_x(self, d):
        return lax.rem(self.x + d, NX)

    def along_y(self, d):
        return lax.rem(self.y + d, NY)

    def along_tp(self, d):
        return lax.rem(self.tp + d, NTP)

    def to_z(self, src, dst):
        out = {}
        for d in Z_ORDER:
            peer = self.along_z(d)
            out[d] = self.send(src(peer), dst, peer * NX + self.x, self.tp)
        return out

    def from_z(self, numbers, dst):
        for d in reversed(Z_ORDER):
            peer = self.along_z(NZ - d)
            self.recv(numbers[d], dst(peer), peer * NX + self.x, self.tp)

    def to_x(self, src, dst):
        out = {}
        for d in (2, 1, 3):
            peer = self.along_x(d)
            out[d] = self.send(src(peer), dst, self.z * NX + peer, self.tp)
        return out

    def from_x(self, numbers, dst):
        for d in (1, 3, 2):
            peer = self.along_x(NX - d)
            self.recv(numbers[d], dst(peer), self.z * NX + peer, self.tp)

    def to_y(self, src, dst):
        out = {}
        for d in (2, 1, 3):
            peer = self.along_y(d)
            out[d] = self.send(src(peer), dst, self.kv, peer * NC + self.c)
        return out

    def from_y(self, numbers, dst):
        for d in (1, 3, 2):
            peer = self.along_y(NY - d)
            self.recv(numbers[d], dst(peer), self.kv, peer * NC + self.c)

    def to_tp(self, src, dst):
        out = {}
        for d in range(1, NTP):
            peer = self.along_tp(d)
            out[d] = self.send(src(peer), dst, self.kv, peer)
        return out

    def from_tp(self, numbers, dst):
        for d in range(1, NTP):
            peer = self.along_tp(NTP - d)
            self.recv(numbers[d], dst(peer), self.kv, peer)


def greet(wire):
    barrier = pltpu.get_barrier_semaphore()

    def tell(kv, tp):
        pl.semaphore_signal(barrier, inc=1, device_id=(kv, tp), device_id_type=MESH)

    for d in range(1, NZ):
        tell(wire.along_z(d) * NX + wire.x, wire.tp)
    for d in range(1, NX):
        tell(wire.z * NX + wire.along_x(d), wire.tp)
    for d in range(1, NTP):
        tell(wire.kv, wire.along_tp(d))
    return lambda: pl.semaphore_wait(barrier, NZ - 1 + NX - 1 + NTP - 1)


def at_rows(start, size, step):
    return pl.ds(pl.multiple_of(start * step, step), size)


def turn_columns(src, dst):
    for j in range(src.shape[1] // 128):
        dst[j * 128 : (j + 1) * 128, :] = src[:, j * 128 : (j + 1) * 128].T


def send_turned(wire, turned, both, at):
    z = wire.z
    lanes = at_rows(z, FEAT, FEAT)
    place = both.at[at : at + CUT, lanes]
    numbers = wire.to_z(lambda peer: turned.at[at_rows(peer, CUT, CUT), :], place)
    both[at : at + CUT, lanes] = turned[at_rows(z, CUT, CUT), :]
    return numbers


def wait_turned(wire, numbers, both, at):
    wire.from_z(numbers, lambda s: both.at[at : at + CUT, at_rows(s, FEAT, FEAT)])


def send_down(wire, down, parts):
    numbers = wire.to_z(lambda peer: down.at[at_rows(peer, CUT, CUT), :], parts.at[wire.z])
    parts[wire.z] = down[at_rows(wire.z, CUT, CUT), :]
    return numbers


def wait_down(wire, numbers, parts, turned):
    wire.from_z(numbers, lambda s: parts.at[s])
    for s in range(NZ):
        turned[s] = parts[s].T


def as_column(row):
    square = jnp.broadcast_to(row, (OWN, OWN))
    same = lax.broadcasted_iota(jnp.int32, (OWN, OWN), 0) == lax.broadcasted_iota(jnp.int32, (OWN, OWN), 1)
    return jnp.sum(jnp.where(same, square, 0.0), axis=1, keepdims=True)


def gather_features(wire, values, gain, feats, sq_z, sq_tp, after_first_sends):
    z, tp, y, c = wire.z, wire.tp, wire.y, wire.c
    sibling = y * NC + (1 - c)
    wide = values.astype(F32)
    feats[z, tp] = (wide * as_column(gain[...])).astype(BF16)
    own = feats.at[z, tp]
    n_feats = {}
    for d in Z_NEAR:
        n_feats[d] = wire.send(own, own, wire.along_z(d) * NX + wire.x, tp)
    n_y, n_core, n_passed = {}, {}, {}

    def hand_on(d, peer):
        block = feats.at[peer, tp]
        n_y[d] = wire.to_y(lambda p: block, block)
        n_core[d] = wire.send(block, block, wire.kv, sibling)

    def pass_on(d, peer):
        for e in (1, 3, 2):
            source = wire.along_y(NY - e) * NC + c
            block = feats.at[peer, source]
            wire.recv(n_y[d][e], block, wire.kv, source)
            n_passed[d, e] = wire.send(block, block, wire.kv, sibling)

    hand_on(0, z)
    sq_z[z] = jnp.sum(wide * wide, axis=0, keepdims=True)
    n_sq = wire.to_z(lambda peer: sq_z.at[z], sq_z.at[z])
    after_first_sends()
    steps = [(0, z)] + [(d, wire.along_z(NZ - d)) for d in Z_NEAR]
    for d, peer in steps[1:]:
        wire.recv(n_feats[d], feats.at[peer, tp], peer * NX + wire.x, tp)
        hand_on(d, peer)
    wire.from_z(n_sq, lambda s: sq_z.at[s])
    sq_tp[tp] = jnp.sum(sq_z[...], axis=0)
    n_sq2 = wire.to_tp(lambda peer: sq_tp.at[tp], sq_tp.at[tp])
    for d, peer in steps:
        pass_on(d, peer)
    wire.from_tp(n_sq2, lambda s: sq_tp.at[s])
    for d, peer in steps:
        wire.recv(n_core[d], feats.at[peer, sibling], wire.kv, sibling)
        for e in (1, 3, 2):
            source = wire.along_y(NY - e) * NC + 1 - c
            wire.recv(n_passed[d, e], feats.at[peer, source], wire.kv, sibling)
    return jnp.sum(sq_tp[...], axis=0)


def channel_mixer(wire, values, gain, s, after_first_sends, wait_weights, wait_down_weights, down_t):
    x = wire.x
    squares = gather_features(wire, values, gain, s["feats"], s["sq_z"], s["sq_tp"], after_first_sends)
    s["sq_x"][x] = squares
    n_sq = wire.to_x(lambda peer: s["sq_x"].at[x], s["sq_x"].at[x])
    wait_weights()
    sums = s["sums"]
    sums[...] = jnp.dot(
        s["both"][...], s["feats"][...].reshape(DEPTH, SEQS), preferred_element_type=F32
    ).astype(BF16)
    sums_x = s["sums_x"]
    n_sums = wire.to_x(lambda peer: sums.at[:, at_rows(peer, XS, XS)], sums_x.at[x])
    sums_x[x] = sums[:, at_rows(x, XS, XS)]
    wire.from_x(n_sq, lambda p: s["sq_x"].at[p])
    s["factor"][...] = lax.rsqrt(jnp.sum(s["sq_x"][...], axis=0) / D + norm_epsilon)
    factor = s["factor"][:, at_rows(x, XS, XS)]
    wire.from_x(n_sums, lambda p: sums_x.at[p])
    gates = sum(sums_x[p, 0:CUT].astype(F32) for p in range(NX)) * factor
    ups = sum(sums_x[p, CUT : 2 * CUT].astype(F32) for p in range(NX)) * factor
    hidden = s["hidden"]
    here = hidden.at[:, at_rows(x, XS, XS)]
    here[...] = (gates / (1.0 + jnp.exp(-gates)) * ups).astype(BF16)
    n_hidden = wire.to_x(lambda peer: here, here)
    wait_down_weights()
    wire.from_x(n_hidden, lambda p: hidden.at[:, at_rows(p, XS, XS)])

    c, y, z = wire.c, wire.y, wire.z
    sibling = y * NC + (1 - c)
    outs, other = s["outs"], s["other"]
    by_y, arrived_y = s["by_y"], s["arrived_y"]
    by_z, arrived_z = s["by_z"], s["arrived_z"]
    order = [(d, wire.along_z(d)) for d in Z_ORDER + (0,)]
    n_core, n_y, n_z = {}, {}, {}
    for d, k in order:
        part = jnp.dot(down_t[k], hidden[...], preferred_element_type=F32)
        outs[k] = part.astype(BF16).reshape(NY, NC, OWN, SEQS)
        n_core[d] = wire.send(outs.at[k, :, 1 - c], other.at[k], wire.kv, sibling)
    for d, k in order:
        wire.recv(n_core[d], other.at[k], wire.kv, sibling)
        by_y[:, k] = (outs[k, :, c].astype(F32) + other[k].astype(F32)).astype(BF16)
        n_y[d] = wire.to_y(lambda peer, k=k: by_y.at[peer, k], arrived_y.at[y, k])
        arrived_y[y, k] = by_y[y, k]
    for d, k in order:
        wire.from_y(n_y[d], lambda p, k=k: arrived_y.at[p, k])
        by_z[k] = sum(arrived_y[p, k].astype(F32) for p in range(NY)).astype(BF16)
        if d:
            n_z[d] = wire.send(by_z.at[k], arrived_z.at[z], k * NX + wire.x, wire.tp)
    arrived_z[z] = by_z[z]
    wire.from_z(n_z, lambda p: arrived_z.at[p])
    return jnp.sum(arrived_z[...].astype(F32), axis=0)


def ff_scratch(name):
    return {
        name + key: value
        for key, value in dict(
            feats=((NZ, NTP, OWN, SEQS), BF16),
            sq_z=((NZ, 1, SEQS), F32),
            sq_tp=((NTP, 1, SEQS), F32),
            sq_x=((NX, 1, SEQS), F32),
            factor=((1, SEQS), F32),
            gate=((FEAT, NZ * CUT), BF16),
            up=((FEAT, NZ * CUT), BF16),
            down=((NZ * CUT, FEAT), BF16),
            gate_t=((NZ * CUT, FEAT), BF16),
            up_t=((NZ * CUT, FEAT), BF16),
            both=((2 * CUT, DEPTH), BF16),
            down_parts=((NZ, CUT, FEAT), BF16),
            down_t=((NZ, FEAT, CUT), BF16),
            sums=((2 * CUT, SEQS), BF16),
            sums_x=((NX, 2 * CUT, XS), BF16),
            hidden=((CUT, SEQS), BF16),
            outs=((NZ, NY, NC, OWN, SEQS), BF16),
            other=((NZ, NY, OWN, SEQS), BF16),
            by_y=((NY, NZ, OWN, SEQS), BF16),
            arrived_y=((NY, NZ, OWN, SEQS), BF16),
            by_z=((NZ, OWN, SEQS), BF16),
            arrived_z=((NZ, OWN, SEQS), BF16),
        ).items()
    }


SCRATCH = dict(
    ff_scratch("a_"),
    **ff_scratch("b_"),
    gate_in=((FEAT, PER * HEAD), BF16),
    value_in=((FEAT, PER * HEAD), BF16),
    write_in=((FEAT, STATE), BF16),
    read_in=((FEAT, STATE), BF16),
    out_weight=((PER * HEAD, FEAT), BF16),
    state=((ROWS, PER, HEAD, STATE), F32),
    conv=((3, ROWS, PER * HEAD + 2 * STATE), BF16),
    mix_t=((NZ, MIX, FEAT), BF16),
    mix_in=((MIX, DEPTH), BF16),
    mix_feats=((NZ, NTP, OWN, SEQS), BF16),
    mix_sq_z=((NZ, 1, SEQS), F32),
    mix_sq_tp=((NTP, 1, SEQS), F32),
    turned=((WIDE, SEQS), F32),
    rows=((NKV, ROWS, WIDE), BF16),
    rows_in=((NKV, ROWS, WIDE), BF16),
    mixed_all=((NZ, NX, ROWS, PER * HEAD), BF16),
    out_t=((NTP, OWN, SEQS), BF16),
    out_in=((NTP, OWN, SEQS), BF16),
)
STAGED = (
    "a_gate",
    "a_up",
    "a_down",
    "gate_in",
    "value_in",
    "write_in",
    "read_in",
    "b_down",
    "b_gate",
    "b_up",
    "state",
    "conv",
    "out_weight",
)
COPIES = 520


def part_of(scratch, name):
    return {key[len(name) :]: ref for key, ref in scratch.items() if key.startswith(name)}


def turn_mixer(s, step_in):
    mix_t = s["mix_t"]
    for j in range(PER * HEAD // 128):
        for ref, at in ((s["gate_in"], 0), (s["value_in"], HEAD)):
            tile = ref[:, j * 128 : (j + 1) * 128].T
            mix_t[2 * j, at : at + HEAD] = tile[:HEAD]
            mix_t[2 * j + 1, at : at + HEAD] = tile[HEAD:]
    for ref, base in ((s["write_in"], 0), (s["read_in"], 4)):
        tile = ref[...].T
        for j in range(4):
            mix_t[base + j, 2 * HEAD : 2 * HEAD + 32] = tile[32 * j : 32 * (j + 1)]
    steps = jnp.concatenate([step_in[...].astype(F32), jnp.zeros((8, FEAT), F32)], axis=0).astype(BF16)
    for j in range(NZ):
        mix_t[j, 2 * HEAD + 32 : MIX] = steps


def silu(v):
    return v / (1.0 + jnp.exp(-v))


def state_step(s, conv_weight, step_bias, log_decay_rate, group_gain, conv_next, decay_out, drive_out, write_out, ready):
    rows_in = s["rows_in"]
    parts = [sum(rows_in[k * NX + p].astype(F32) for p in range(NX)) for k in range(NZ)]
    factor = lax.rsqrt(parts[3][:, 2 * HEAD + 8 : 2 * HEAD + 9] / D + norm_epsilon)
    parts = [(part * factor).astype(BF16).astype(F32) for part in parts]
    lane = lax.broadcasted_iota(jnp.int32, (ROWS, 128), 1)
    low = lane < HEAD
    gates, values, writes, reads = [], [], 0.0, 0.0
    for j in range(PER // 2):
        a, b = parts[2 * j][:, :128], parts[2 * j + 1][:, :128]
        gates.append(jnp.where(low, a, pltpu.roll(b, HEAD, 1)))
        values.append(jnp.where(low, pltpu.roll(a, HEAD, 1), b))
    for k in range(4):
        here = lane // 32 == k
        writes = writes + jnp.where(here, parts[k][:, 128:], 0.0)
        reads = reads + jnp.where(here, parts[4 + k][:, 128:], 0.0)
    gate = jnp.concatenate(gates, axis=1)
    fresh = jnp.concatenate([*values, writes, reads], axis=1)
    ready()
    conv = s["conv"]
    conv_next[0] = conv[1]
    conv_next[1] = conv[2]
    conv_next[2] = fresh.astype(BF16)
    total = fresh * conv_weight[3]
    for t in range(3):
        total = total + conv[t].astype(F32) * conv_weight[t]
    activated = silu(total)
    inputs = activated[:, : PER * HEAD]
    write_vec = activated[:, PER * HEAD : PER * HEAD + STATE]
    read_vec = activated[:, PER * HEAD + STATE :]
    raw_step = parts[3][:, 128 : 128 + PER] + step_bias[...]
    step_size = jnp.maximum(raw_step, 0.0) + jnp.log1p(jnp.exp(-jnp.abs(raw_step)))
    decay = jnp.exp(-step_size * jnp.exp(log_decay_rate[...]))

    def over_heads(v):
        return jnp.concatenate(
            [jnp.where(low, v[:, 2 * j : 2 * j + 1], v[:, 2 * j + 1 : 2 * j + 2]) for j in range(PER // 2)],
            axis=1,
        )

    drive = over_heads(step_size) * inputs
    decay_out[...] = decay
    drive_out[...] = drive
    write_out[...] = write_vec
    row = lax.broadcasted_iota(jnp.int32, (ROWS, STATE), 0)
    state = s["state"]
    carried = 0.0
    for b in range(ROWS):
        one = jnp.where(row == b, read_vec, 0.0).astype(BF16)
        flat = state[b].reshape(PER * HEAD, STATE).astype(BF16)
        carried = carried + lax.dot_general(one, flat, (((1,), (1,)), ((), ())), preferred_element_type=F32)
    readout = over_heads(decay) * carried + drive * jnp.sum(write_vec * read_vec, axis=1, keepdims=True)
    gated = readout * silu(gate)
    scale = lax.rsqrt(jnp.mean(gated * gated, axis=1, keepdims=True) + norm_epsilon)
    return (gated * scale * group_gain[...]).astype(BF16)


def layer(*refs):
    (stream, gain_1, gain_2, gain_3, step_in, conv_weight, step_bias, log_decay_rate, group_gain) = refs[:9]
    held = dict(zip(STAGED, refs[9 : 9 + len(STAGED)]))
    refs = refs[9 + len(STAGED) :]
    result, conv_next, decay_out, drive_out, write_out = refs[:5]
    refs = refs[5:]
    s = dict(zip(SCRATCH, refs))
    sends, recvs, row_sends, row_recvs, stage_sems = refs[len(SCRATCH) :]
    wire = Wire(sends, recvs)
    z, x, kv, tp = wire.z, wire.x, wire.kv, wire.tp
    wait_greeting = greet(wire)

    staging = {
        name: pltpu.make_async_copy(held[name], s[name], stage_sems.at[i]) for i, name in enumerate(STAGED)
    }
    for copy in staging.values():
        copy.start()
    a, b = part_of(s, "a_"), part_of(s, "b_")
    staging["a_gate"].wait()
    turn_columns(a["gate"], a["gate_t"])
    staging["a_up"].wait()
    turn_columns(a["up"], a["up_t"])
    wait_greeting()
    numbers = {}

    def weights_out():
        numbers["gate"] = send_turned(wire, a["gate_t"], a["both"], 0)
        numbers["up"] = send_turned(wire, a["up_t"], a["both"], CUT)
        staging["a_down"].wait()
        numbers["down"] = send_down(wire, a["down"], a["down_parts"])
        for name in ("gate_in", "value_in", "write_in", "read_in"):
            staging[name].wait()
        turn_mixer(s, step_in)
        lanes = at_rows(z, FEAT, FEAT)
        numbers["mix"] = wire.to_z(lambda peer: s["mix_t"].at[peer], s["mix_in"].at[:, lanes])
        s["mix_in"][:, lanes] = s["mix_t"][z]

    def first_weights():
        staging["b_gate"].wait()
        turn_columns(b["gate"], b["gate_t"])
        staging["b_up"].wait()
        turn_columns(b["up"], b["up_t"])
        wait_turned(wire, numbers["gate"], a["both"], 0)
        wait_turned(wire, numbers["up"], a["both"], CUT)

    branch = channel_mixer(
        wire,
        stream[...],
        gain_1,
        a,
        weights_out,
        first_weights,
        lambda: wait_down(wire, numbers["down"], a["down_parts"], a["down_t"]),
        a["down_t"],
    )
    after = (stream[...].astype(F32) + 0.5 * branch).astype(BF16)

    def next_down():
        staging["b_down"].wait()
        numbers["next_down"] = send_down(wire, b["down"], b["down_parts"])

    squares = gather_features(wire, after, gain_2, s["mix_feats"], s["mix_sq_z"], s["mix_sq_tp"], next_down)
    wire.from_z(numbers["mix"], lambda p: s["mix_in"].at[:, at_rows(p, FEAT, FEAT)])
    part = jnp.dot(s["mix_in"][...], s["mix_feats"][...].reshape(DEPTH, SEQS), preferred_element_type=F32)
    turned = s["turned"]
    turned[2 * HEAD :, :] = jnp.zeros((WIDE - 2 * HEAD, SEQS), F32)
    turned[: 2 * HEAD, :] = part[: 2 * HEAD]
    quarter = lax.rem(z, 4)
    turned[pl.ds(pl.multiple_of(128 + 32 * quarter, 32), 32), :] = part[2 * HEAD : 2 * HEAD + 32]
    beside = pl.multiple_of(128 + 32 * lax.rem(z + 1, 4), 32)
    turned[pl.ds(beside, 8), :] = part[2 * HEAD + 32 : 2 * HEAD + 40]
    turned[pl.ds(pl.multiple_of(beside + 8, 8), 8), :] = jnp.broadcast_to(squares, (8, SEQS))
    rows, rows_in = s["rows"], s["rows_in"]
    rows[...] = turned[...].T.astype(BF16).reshape(NKV, ROWS, WIDE)

    def row_copy(d, peer, slot):
        return pltpu.make_async_remote_copy(
            src_ref=rows.at[peer],
            dst_ref=rows_in.at[slot],
            send_sem=row_sends.at[d],
            recv_sem=row_recvs.at[d],
            device_id=(peer, tp),
            device_id_type=MESH,
        )

    @pl.loop(1, NKV)
    def _(d):
        row_copy(d, lax.rem(kv + d, NKV), kv).start()

    rows_in[kv] = rows[kv]
    numbers["next_gate"] = send_turned(wire, b["gate_t"], b["both"], 0)
    staging["state"].wait()

    @pl.loop(1, NKV)
    def _(d):
        peer = lax.rem(kv + NKV - d, NKV)
        row_copy(d, peer, peer).wait_recv()

    mixed = state_step(
        s,
        conv_weight,
        step_bias,
        log_decay_rate,
        group_gain,
        conv_next,
        decay_out,
        drive_out,
        write_out,
        lambda: staging["conv"].wait(),
    )

    mixed_all = s["mixed_all"]
    mixed_all[z, x] = mixed
    own = mixed_all.at[z, x]
    n_z, n_x = {}, {}
    for d in Z_NEAR:
        n_z[d] = wire.send(own, own, wire.along_z(d) * NX + x, tp)
    n_x[0] = wire.to_x(lambda peer: own, own)
    numbers["next_up"] = send_turned(wire, b["up_t"], b["both"], CUT)
    staging["out_weight"].wait()
    steps = [(0, z)] + [(d, wire.along_z(NZ - d)) for d in Z_NEAR]
    for d, peer in steps[1:]:
        block = mixed_all.at[peer, x]
        wire.recv(n_z[d], block, peer * NX + x, tp)
        n_x[d] = wire.to_x(lambda p, block=block: block, block)
    for d, peer in steps:
        wire.from_x(n_x[d], lambda p, peer=peer: mixed_all.at[peer, p])
    part = jnp.dot(mixed_all[...].reshape(SEQS, PER * HEAD), s["out_weight"][...], preferred_element_type=F32)
    out_t, out_in = s["out_t"], s["out_in"]
    out_t[...] = part.T.astype(BF16).reshape(NTP, OWN, SEQS)
    n_tp = wire.to_tp(lambda peer: out_t.at[peer], out_in.at[tp])
    out_in[tp] = out_t[tp]
    wire.from_tp(n_tp, lambda p: out_in.at[p])
    after = (after.astype(F32) + jnp.sum(out_in[...].astype(F32), axis=0)).astype(BF16)

    def second_weights():
        wait_turned(wire, numbers["next_gate"], b["both"], 0)
        wait_turned(wire, numbers["next_up"], b["both"], CUT)

    branch = channel_mixer(
        wire,
        after,
        gain_3,
        b,
        lambda: wait_down(wire, numbers["next_down"], b["down_parts"], b["down_t"]),
        second_weights,
        lambda: None,
        b["down_t"],
    )
    result[...] = (after.astype(F32) + 0.5 * branch).astype(BF16)
    wire.drain()

    @pl.loop(1, NKV)
    def _(d):
        row_copy(d, lax.rem(kv + d, NKV), kv).wait_send()


def on_device(
    stream,
    ssm_state,
    conv_state,
    first_gain,
    first_gate,
    first_up,
    first_down,
    mix_gain,
    gate_in,
    value_in,
    write_in,
    read_in,
    step_in,
    conv_weight,
    step_bias,
    log_decay_rate,
    group_gain,
    out_weight,
    last_norm_gain,
    second_gate,
    second_up,
    second_down,
):
    staged = dict(
        a_gate=first_gate,
        a_up=first_up,
        a_down=first_down,
        gate_in=gate_in,
        value_in=value_in,
        write_in=write_in,
        read_in=read_in,
        b_down=second_down,
        b_gate=second_gate,
        b_up=second_up,
        state=ssm_state,
        conv=conv_state[:, :, 0].transpose(1, 0, 2),
        out_weight=out_weight,
    )
    small = (
        stream.T,
        first_gain[None],
        mix_gain[None],
        last_norm_gain[None],
        step_in.T,
        conv_weight,
        step_bias[None],
        log_decay_rate[None],
        group_gain[None],
    )
    whole = pl.BlockSpec(memory_space=pltpu.VMEM)
    outs = (
        jax.ShapeDtypeStruct((OWN, SEQS), BF16),
        jax.ShapeDtypeStruct((3, ROWS, PER * HEAD + 2 * STATE), BF16),
        jax.ShapeDtypeStruct((ROWS, PER), F32),
        jax.ShapeDtypeStruct((ROWS, PER * HEAD), F32),
        jax.ShapeDtypeStruct((ROWS, STATE), F32),
    )
    result, conv_next, decay, drive, write_vec = pl.pallas_call(
        layer,
        name="layer",
        out_shape=outs,
        in_specs=[whole] * len(small) + [pl.BlockSpec(memory_space=pl.ANY)] * len(STAGED),
        out_specs=[whole] * len(outs),
        scratch_shapes=[pltpu.VMEM(shape, dtype) for shape, dtype in SCRATCH.values()]
        + [pltpu.SemaphoreType.DMA((COPIES,))] * 2
        + [pltpu.SemaphoreType.DMA((NKV,))] * 2
        + [pltpu.SemaphoreType.DMA((len(STAGED),))],
        compiler_params=pltpu.CompilerParams(
            collective_id=0, has_side_effects=True, vmem_limit_bytes=60 * 1024 * 1024
        ),
    )(*small, *(staged[name] for name in STAGED))
    ssm_next = (
        ssm_state * decay[:, :, None, None]
        + drive.reshape(ROWS, PER, HEAD)[..., None] * write_vec[:, None, None, :]
    )
    return (result.T, ssm_next, conv_next.transpose(1, 0, 2)[:, :, None])


def solution(mesh):
    placed = (
        P(None, ("kv", "tp")),
        P("kv", "tp", None, None),
        P("kv", None, "tp", None),
        P(("kv", "tp")),
        P("kv", "tp"),
        P("kv", "tp"),
        P("tp", "kv"),
        P(("kv", "tp")),
        P("kv", "tp"),
        P("kv", "tp"),
        P("kv", "tp"),
        P("kv", "tp"),
        P("kv", "tp"),
        P(None, "tp", None),
        P("tp"),
        P("tp"),
        P("tp"),
        P("tp", "kv"),
        P(("kv", "tp")),
        P("kv", "tp"),
        P("kv", "tp"),
        P("tp", "kv"),
    )
    return jax.shard_map(
        on_device,
        mesh=mesh,
        in_specs=placed,
        out_specs=(P(None, ("kv", "tp")), P("kv", "tp", None, None), P("kv", None, "tp", None)),
        check_vma=False,
    )
```

```python
import jax
import jax.numpy as jnp
from jax import lax
from jax.experimental import pallas as pl
from jax.experimental.pallas import tpu as pltpu
from jax.sharding import PartitionSpec as P

MESH = pl.DeviceIdType.MESH
F32, BF16 = jnp.float32, jnp.bfloat16

NZ, NX, NY, NC = 8, 4, 4, 2
NKV, NTP = NZ * NX, NY * NC
SEQS, D, FF = 512, 4096, 11264
OWN = D // (NKV * NTP)
FEAT = OWN * NTP
DEPTH = FEAT * NZ
CUT = FF // NTP // NZ
XS = SEQS // NX
ROWS = SEQS // NKV
HEAD, STATE, PER = 64, 128, 8
MIX = 176
WIDE = 256
PARTS = ((0, 96), (96, 80))
norm_epsilon = 1e-06


class Wire:
    def __init__(self, sends, recvs):
        self.sends, self.recvs, self.n_sends, self.n_recvs, self.pending = sends, recvs, 0, 0, []
        kv, self.tp = lax.axis_index("kv"), lax.axis_index("tp")
        self.kv = kv
        self.z, self.x = lax.div(kv, NX), lax.rem(kv, NX)
        self.y, self.c = lax.div(self.tp, NC), lax.rem(self.tp, NC)
        self.sibling = self.y * NC + (1 - self.c)

    def along_y(self, d):
        return lax.rem(self.y + d, NY)

    def along_tp(self, d):
        return lax.rem(self.tp + d, NTP)

    def settle(self, keep=()):
        for copies in self.pending:
            if copies not in keep:
                copies.left()
        self.pending = [copies for copies in self.pending if copies in keep]


class Copies:
    def __init__(self, wire, every, pending=True):
        self.wire, self.every, self.keys = wire, every, {}
        self.sem = wire.sends.at[wire.n_sends]
        wire.n_sends += 1
        if pending:
            wire.pending.append(self)

    def arrival(self, key):
        if key not in self.keys:
            self.keys[key] = self.wire.n_recvs
            self.wire.n_recvs += 1
        return self.wire.recvs.at[self.keys[key]]

    def _copy(self, src, dst, kv, tp, key):
        return pltpu.make_async_remote_copy(
            src_ref=src,
            dst_ref=dst,
            send_sem=self.sem,
            recv_sem=self.arrival(key),
            device_id=(kv, tp),
            device_id_type=MESH,
        )

    def send(self, src, dst, kv, tp, key=0):
        self._copy(src, dst, kv, tp, key).start()

    def arrived(self, whole, key=0):
        self._copy(whole, whole, self.wire.kv, self.wire.sibling, key).wait_recv()

    def left(self):
        self._copy(self.every, self.every, self.wire.kv, self.wire.sibling, next(iter(self.keys))).wait_send()

    def to_y(self, src, dst, key=0):
        wire = self.wire
        for d in (2, 1, 3):
            peer = wire.along_y(d)
            self.send(src(peer), dst, wire.kv, peer * NC + wire.c, key)

    def to_tp(self, src, dst):
        for d in range(1, NTP):
            peer = self.wire.along_tp(d)
            self.send(src(peer), dst, self.wire.kv, peer)

    def to_g(self, plane, src, dst):
        for d in plane.far:
            peer = plane.ahead(d)
            self.send(src(peer), dst, plane.kv_at(peer, plane.h), self.wire.tp)

    def to_h(self, plane, src, dst, key=0):
        for d in (2, 1, 3):
            peer = lax.rem(plane.h + d, NX)
            self.send(src(peer), dst, plane.kv_at(plane.g, peer), self.wire.tp, key)


class Plane:
    def __init__(self, wire, folded):
        self.folded = folded
        if folded:
            self.g, self.h = wire.x + NX * lax.rem(wire.z, 2), lax.div(wire.z, 2)
            self.near = (1, 3, 4, 5, 7, 2, 6)
        else:
            self.g, self.h = wire.z, wire.x
            self.near = (1, 7, 2, 6, 3, 5, 4)
        self.far = self.near[::-1]

    def kv_at(self, g, h):
        if self.folded:
            if isinstance(g, int) and isinstance(h, int):
                return (2 * h + g // NX) * NX + g % NX
            return (2 * h + lax.div(g, NX)) * NX + lax.rem(g, NX)
        return g * NX + h

    def ahead(self, d):
        if not self.folded:
            return lax.rem(self.g + d, NZ)
        x, pair = lax.rem(self.g, NX), lax.div(self.g, NX)
        return lax.rem(x + d % NX, NX) + NX * lax.rem(pair + d // NX, 2)

    def behind(self, d):
        if not self.folded:
            return lax.rem(self.g + NZ - d, NZ)
        x, pair = lax.rem(self.g, NX), lax.div(self.g, NX)
        return lax.rem(x + NX - d % NX, NX) + NX * lax.rem(pair + d // NX, 2)


def greet(wire):
    barrier = pltpu.get_barrier_semaphore()

    def tell(kv, tp):
        pl.semaphore_signal(barrier, inc=1, device_id=(kv, tp), device_id_type=MESH)

    for d in range(1, NZ):
        tell(lax.rem(wire.z + d, NZ) * NX + wire.x, wire.tp)
    for d in range(1, NX):
        x = lax.rem(wire.x + d, NX)
        tell(wire.z * NX + x, wire.tp)
        tell((wire.z + 1 - 2 * lax.rem(wire.z, 2)) * NX + x, wire.tp)
    for d in range(1, NTP):
        tell(wire.kv, wire.along_tp(d))
    return lambda: pl.semaphore_wait(barrier, NZ - 1 + 2 * (NX - 1) + NTP - 1)


def at_rows(start, size, step):
    return pl.ds(pl.multiple_of(start * step, step), size)


def turn_columns(src, dst):
    for j in range(src.shape[1] // 128):
        dst[j * 128 : (j + 1) * 128, :] = src[:, j * 128 : (j + 1) * 128].T


def send_gate_up(wire, plane, gate_t, up_t, both, part):
    g = plane.g
    lanes = at_rows(g, FEAT, FEAT)
    start, size = PARTS[part]
    out = []
    for turned, at in ((gate_t, 2 * start), (up_t, 2 * start + size)):
        copies = Copies(wire, both.at[at : at + size, 0 : (NZ - 1) * FEAT], False)

        def cut(peer):
            return pl.ds(pl.multiple_of(peer * CUT + start, OWN), size)

        copies.to_g(plane, lambda peer: turned.at[cut(peer), :], both.at[at : at + size, lanes])
        both[at : at + size, lanes] = turned[cut(g), :]
        out.append(copies)
    return out


def wait_all(sets):
    for copies in sets:
        copies.arrived(copies.every)


def send_down(wire, plane, down, parts):
    g = plane.g
    copies = Copies(wire, parts.at[0 : NZ - 1], False)
    copies.to_g(plane, lambda peer: down.at[at_rows(peer, CUT, CUT), :], parts.at[g])
    parts[g] = down[at_rows(g, CUT, CUT), :]
    return copies


def wait_down(copies, parts, turned):
    copies.arrived(copies.every)
    for s in range(NZ):
        turned[s] = parts[s].T


def silu(v):
    return v / (1.0 + jnp.exp(-v))


def as_column(row):
    square = jnp.broadcast_to(row, (OWN, OWN))
    same = lax.broadcasted_iota(jnp.int32, (OWN, OWN), 0) == lax.broadcasted_iota(jnp.int32, (OWN, OWN), 1)
    return jnp.sum(jnp.where(same, square, 0.0), axis=1, keepdims=True)


def gather_features(wire, plane, values, gain, feats, sq_g, sq_tp, after_first_sends):
    g, tp, c, sibling = plane.g, wire.tp, wire.c, wire.sibling
    wide = values.astype(F32)
    feats[g, tp] = (wide * as_column(gain[...])).astype(BF16)
    own = feats.at[g, tp]
    to_group = Copies(wire, feats.at[0, 0 : NZ - 1])
    for d in plane.near:
        to_group.send(own, own, plane.kv_at(plane.ahead(d), plane.h), tp, d)
    along = Copies(wire, feats.at[0 : NY - 1])
    across = Copies(wire, feats.at[0:NY])

    def hand_on(d, peer):
        block = feats.at[peer, tp]
        along.to_y(lambda p: block, block, d)
        across.send(block, block, wire.kv, sibling)

    hand_on(0, g)
    sq_g[g] = jnp.sum(wide * wide, axis=0, keepdims=True)
    squares_g = Copies(wire, sq_g.at[0 : NZ - 1])
    squares_g.to_g(plane, lambda peer: sq_g.at[g], sq_g.at[g])
    after_first_sends()
    steps = [(0, g)] + [(d, plane.behind(d)) for d in plane.near]
    for d, peer in steps[1:]:
        to_group.arrived(feats.at[peer, tp], d)
        hand_on(d, peer)
    squares_g.arrived(squares_g.every)
    sq_tp[tp] = jnp.sum(sq_g[...], axis=0)
    squares_tp = Copies(wire, sq_tp.at[0 : NTP - 1])
    squares_tp.to_tp(lambda peer: sq_tp.at[tp], sq_tp.at[tp])
    for d, peer in steps:
        along.arrived(feats.at[peer, 0 : NY - 1], d)
        for e in (1, 3, 2):
            block = feats.at[peer, wire.along_y(NY - e) * NC + c]
            across.send(block, block, wire.kv, sibling)
    squares_tp.arrived(squares_tp.every)
    across.arrived(across.every)
    return jnp.sum(sq_tp[...], axis=0)


def channel_mixer(wire, plane, values, gain, s, after_first_sends, wait_weights, after_hidden, down_t):
    g, h = plane.g, plane.h
    squares = gather_features(wire, plane, values, gain, s["feats"], s["sq_g"], s["sq_tp"], after_first_sends)
    sq_h, sums, sums_h, hidden = s["sq_h"], s["sums"], s["sums_h"], s["hidden"]
    sq_h[h] = squares
    squares_h = Copies(wire, sq_h.at[0 : NX - 1])
    squares_h.to_h(plane, lambda peer: sq_h.at[h], sq_h.at[h])
    gathered = list(wire.pending)
    sums_out = []
    for part, (start, size) in enumerate(PARTS):
        wait_weights(part)
        rows = slice(2 * start, 2 * (start + size))
        sums[rows] = jnp.dot(
            s["both"][rows], s["feats"][...].reshape(DEPTH, SEQS), preferred_element_type=F32
        ).astype(BF16)
        copies = Copies(wire, sums_h.at[0 : NX - 1, rows])
        copies.to_h(plane, lambda peer: sums.at[rows, at_rows(peer, XS, XS)], sums_h.at[h, rows])
        sums_h[h, rows] = sums[rows, at_rows(h, XS, XS)]
        sums_out.append(copies)
    squares_h.arrived(squares_h.every)
    s["factor"][...] = lax.rsqrt(jnp.sum(sq_h[...], axis=0) / D + norm_epsilon)
    factor = s["factor"][:, at_rows(h, XS, XS)]
    hidden_out = []
    for (start, size), copies in zip(PARTS, sums_out):
        copies.arrived(copies.every)
        at = 2 * start
        gates = sum(sums_h[p, at : at + size].astype(F32) for p in range(NX)) * factor
        ups = sum(sums_h[p, at + size : at + 2 * size].astype(F32) for p in range(NX)) * factor
        here = hidden.at[start : start + size, at_rows(h, XS, XS)]
        here[...] = (silu(gates) * ups).astype(BF16)
        out = Copies(wire, hidden.at[start : start + size, 0 : SEQS - XS])
        out.to_h(plane, lambda peer: here, here)
        hidden_out.append(out)
    after_hidden()
    for copies in gathered:
        copies.left()
    wire.pending = [copies for copies in wire.pending if copies not in gathered]
    wait_all(hidden_out)

    c, y = wire.c, wire.y
    outs, other = s["outs"], s["other"]
    by_y, arrived_y = s["by_y"], s["arrived_y"]
    by_g, arrived_g = s["by_g"], s["arrived_g"]
    order = [(d, plane.ahead(d)) for d in plane.far + (0,)]
    across, along = Copies(wire, other), Copies(wire, by_y.at[0 : NY - 1])
    to_group = Copies(wire, by_g.at[0 : NZ - 1])
    for d, k in order:
        part = jnp.dot(down_t[k], hidden[...], preferred_element_type=F32)
        outs[k] = part.astype(BF16).reshape(NY, NC, OWN, SEQS)
        across.send(outs.at[k, :, 1 - c], other.at[k], wire.kv, wire.sibling, d)
    for d, k in order:
        across.arrived(other.at[k], d)
        by_y[:, k] = (outs[k, :, c].astype(F32) + other[k].astype(F32)).astype(BF16)
        along.to_y(lambda peer: by_y.at[peer, k], arrived_y.at[y, k], d)
        arrived_y[y, k] = by_y[y, k]
    for d, k in order:
        along.arrived(arrived_y.at[0 : NY - 1, k], d)
        by_g[k] = sum(arrived_y[p, k].astype(F32) for p in range(NY)).astype(BF16)
        if d:
            to_group.send(by_g.at[k], arrived_g.at[g], plane.kv_at(k, h), wire.tp)
    arrived_g[g] = by_g[g]
    wire.settle((to_group,))
    to_group.arrived(to_group.every)
    return jnp.sum(arrived_g[...].astype(F32), axis=0)


def ff_scratch(name):
    return {
        name + key: value
        for key, value in dict(
            feats=((NZ, NTP, OWN, SEQS), BF16),
            sq_g=((NZ, 1, SEQS), F32),
            sq_tp=((NTP, 1, SEQS), F32),
            sq_h=((NX, 1, SEQS), F32),
            factor=((1, SEQS), F32),
            gate=((FEAT, NZ * CUT), BF16),
            up=((FEAT, NZ * CUT), BF16),
            down=((NZ * CUT, FEAT), BF16),
            gate_t=((NZ * CUT, FEAT), BF16),
            up_t=((NZ * CUT, FEAT), BF16),
            both=((2 * CUT, DEPTH), BF16),
            down_parts=((NZ, CUT, FEAT), BF16),
            down_t=((NZ, FEAT, CUT), BF16),
            sums=((2 * CUT, SEQS), BF16),
            sums_h=((NX, 2 * CUT, XS), BF16),
            hidden=((CUT, SEQS), BF16),
            outs=((NZ, NY, NC, OWN, SEQS), BF16),
            other=((NZ, NY, OWN, SEQS), BF16),
            by_y=((NY, NZ, OWN, SEQS), BF16),
            arrived_y=((NY, NZ, OWN, SEQS), BF16),
            by_g=((NZ, OWN, SEQS), BF16),
            arrived_g=((NZ, OWN, SEQS), BF16),
        ).items()
    }


SCRATCH = dict(
    ff_scratch("a_"),
    **ff_scratch("b_"),
    gate_in=((FEAT, PER * HEAD), BF16),
    value_in=((FEAT, PER * HEAD), BF16),
    write_in=((FEAT, STATE), BF16),
    read_in=((FEAT, STATE), BF16),
    out_weight=((PER * HEAD, FEAT), BF16),
    state=((ROWS, PER, HEAD, STATE), F32),
    conv=((3, ROWS, PER * HEAD + 2 * STATE), BF16),
    mix_t=((NZ, MIX, FEAT), BF16),
    mix_in=((MIX, DEPTH), BF16),
    mix_feats=((NZ, NTP, OWN, SEQS), BF16),
    mix_sq_g=((NZ, 1, SEQS), F32),
    mix_sq_tp=((NTP, 1, SEQS), F32),
    turned=((WIDE, SEQS), F32),
    rows=((NKV, ROWS, WIDE), BF16),
    rows_in=((NKV, ROWS, WIDE), BF16),
    mixed_all=((NZ, NX, ROWS, PER * HEAD), BF16),
    out_t=((NTP, OWN, SEQS), BF16),
    out_in=((NTP, OWN, SEQS), BF16),
)
STAGED = (
    "a_gate",
    "a_up",
    "a_down",
    "gate_in",
    "value_in",
    "write_in",
    "read_in",
    "b_down",
    "b_gate",
    "b_up",
    "state",
    "conv",
    "out_weight",
)
LEAVE, ARRIVE = 56, 136
VMEM_LIMIT = 58 * 1024 * 1024


def part_of(scratch, name):
    return {key[len(name) :]: ref for key, ref in scratch.items() if key.startswith(name)}


def turn_mixer(s, step_in):
    mix_t = s["mix_t"]
    for j in range(PER * HEAD // 128):
        for ref, at in ((s["gate_in"], 0), (s["value_in"], HEAD)):
            tile = ref[:, j * 128 : (j + 1) * 128].T
            mix_t[2 * j, at : at + HEAD] = tile[:HEAD]
            mix_t[2 * j + 1, at : at + HEAD] = tile[HEAD:]
    for ref, base in ((s["write_in"], 0), (s["read_in"], 4)):
        tile = ref[...].T
        for j in range(4):
            mix_t[base + j, 2 * HEAD : 2 * HEAD + 32] = tile[32 * j : 32 * (j + 1)]
    steps = jnp.concatenate([step_in[...].astype(F32), jnp.zeros((8, FEAT), F32)], axis=0).astype(BF16)
    for j in range(NZ):
        mix_t[j, 2 * HEAD + 32 : MIX] = steps


def state_step(s, plane, conv_weight, step_bias, log_decay_rate, group_gain, conv_next, state, ready):
    rows_in = s["rows_in"]
    parts = [sum(rows_in[plane.kv_at(k, p)].astype(F32) for p in range(NX)) for k in range(NZ)]
    factor = lax.rsqrt(parts[3][:, 2 * HEAD + 8 : 2 * HEAD + 9] / D + norm_epsilon)
    parts = [(part * factor).astype(BF16).astype(F32) for part in parts]
    lane = lax.broadcasted_iota(jnp.int32, (ROWS, 128), 1)
    low = lane < HEAD
    gates, values, writes, reads = [], [], 0.0, 0.0
    for j in range(PER // 2):
        a, b = parts[2 * j][:, :128], parts[2 * j + 1][:, :128]
        gates.append(jnp.where(low, a, pltpu.roll(b, HEAD, 1)))
        values.append(jnp.where(low, pltpu.roll(a, HEAD, 1), b))
    for k in range(4):
        here = lane // 32 == k
        writes = writes + jnp.where(here, parts[k][:, 128:], 0.0)
        reads = reads + jnp.where(here, parts[4 + k][:, 128:], 0.0)
    gate = jnp.concatenate(gates, axis=1)
    fresh = jnp.concatenate([*values, writes, reads], axis=1)
    ready()
    conv = s["conv"]
    conv_next[0] = conv[1]
    conv_next[1] = conv[2]
    conv_next[2] = fresh.astype(BF16)
    total = fresh * conv_weight[3]
    for t in range(3):
        total = total + conv[t].astype(F32) * conv_weight[t]
    activated = silu(total)
    inputs = activated[:, : PER * HEAD]
    write_vec = activated[:, PER * HEAD : PER * HEAD + STATE]
    read_vec = activated[:, PER * HEAD + STATE :]
    raw_step = parts[3][:, 128 : 128 + PER] + step_bias[...]
    step_size = jnp.maximum(raw_step, 0.0) + jnp.log1p(jnp.exp(-jnp.abs(raw_step)))
    decay = jnp.exp(-step_size * jnp.exp(log_decay_rate[...]))

    def over_heads(v):
        return jnp.concatenate(
            [jnp.where(low, v[:, 2 * j : 2 * j + 1], v[:, 2 * j + 1 : 2 * j + 2]) for j in range(PER // 2)],
            axis=1,
        )

    drive, kept = over_heads(step_size) * inputs, over_heads(decay)
    row = lax.broadcasted_iota(jnp.int32, (ROWS, STATE), 0)
    carried = 0.0
    for b in range(ROWS):
        one = jnp.where(row == b, read_vec, 0.0).astype(BF16)
        flat = state[b].reshape(PER * HEAD, STATE).astype(BF16)
        carried = carried + lax.dot_general(one, flat, (((1,), (1,)), ((), ())), preferred_element_type=F32)
    readout = kept * carried + drive * jnp.sum(write_vec * read_vec, axis=1, keepdims=True)
    gated = readout * silu(gate)
    scale = lax.rsqrt(jnp.mean(gated * gated, axis=1, keepdims=True) + norm_epsilon)
    return (gated * scale * group_gain[...]).astype(BF16), (kept, drive, write_vec)


def layer(*refs):
    (stream, gain_1, gain_2, gain_3, step_in, conv_weight, step_bias, log_decay_rate, group_gain) = refs[:9]
    held = dict(zip(STAGED, refs[9 : 9 + len(STAGED)]))
    refs = refs[9 + len(STAGED) :]
    result, conv_next, kept_out, drive_out, write_out = refs[:5]
    refs = refs[5:]
    s = dict(zip(SCRATCH, refs))
    sends, recvs, stage_sems = refs[len(SCRATCH) :]
    wire = Wire(sends, recvs)
    plain, folded = Plane(wire, False), Plane(wire, True)
    z, x, kv, tp = wire.z, wire.x, wire.kv, wire.tp
    wait_greeting = greet(wire)

    staging = {
        name: pltpu.make_async_copy(held[name], s[name], stage_sems.at[i]) for i, name in enumerate(STAGED)
    }
    for copy in staging.values():
        copy.start()
    a, b = part_of(s, "a_"), part_of(s, "b_")
    staging["a_gate"].wait()
    turn_columns(a["gate"], a["gate_t"])
    staging["a_up"].wait()
    turn_columns(a["up"], a["up_t"])
    wait_greeting()
    sets = {}

    def weights_out():
        sets["first"] = [send_gate_up(wire, folded, a["gate_t"], a["up_t"], a["both"], part) for part in (0, 1)]
        staging["a_down"].wait()
        sets["down"] = send_down(wire, folded, a["down"], a["down_parts"])
        for name in ("gate_in", "value_in", "write_in", "read_in"):
            staging[name].wait()
        turn_mixer(s, step_in)

    def first_weights(part):
        if part == 0:
            staging["b_gate"].wait()
            turn_columns(b["gate"], b["gate_t"])
            staging["b_up"].wait()
            turn_columns(b["up"], b["up_t"])
        wait_all(sets["first"][part])

    def after_first_hidden():
        lanes = at_rows(folded.g, FEAT, FEAT)
        sets["mix"] = Copies(wire, s["mix_in"].at[:, 0 : (NZ - 1) * FEAT], False)
        sets["mix"].to_g(folded, lambda peer: s["mix_t"].at[peer], s["mix_in"].at[:, lanes])
        s["mix_in"][:, lanes] = s["mix_t"][folded.g]
        staging["b_down"].wait()
        sets["next_down"] = send_down(wire, plain, b["down"], b["down_parts"])
        wait_down(sets["down"], a["down_parts"], a["down_t"])

    branch = channel_mixer(
        wire, folded, stream[...], gain_1, a, weights_out, first_weights, after_first_hidden, a["down_t"]
    )
    after = (stream[...].astype(F32) + 0.5 * branch).astype(BF16)

    def next_gate():
        sets["second"] = [send_gate_up(wire, plain, b["gate_t"], b["up_t"], b["both"], 0)]

    squares = gather_features(
        wire, folded, after, gain_2, s["mix_feats"], s["mix_sq_g"], s["mix_sq_tp"], next_gate
    )
    wait_all([sets["mix"]])
    part = jnp.dot(s["mix_in"][...], s["mix_feats"][...].reshape(DEPTH, SEQS), preferred_element_type=F32)
    turned = s["turned"]
    turned[2 * HEAD :, :] = jnp.zeros((WIDE - 2 * HEAD, SEQS), F32)
    turned[: 2 * HEAD, :] = part[: 2 * HEAD]
    quarter = lax.rem(folded.g, 4)
    turned[pl.ds(pl.multiple_of(128 + 32 * quarter, 32), 32), :] = part[2 * HEAD : 2 * HEAD + 32]
    beside = pl.multiple_of(128 + 32 * lax.rem(folded.g + 1, 4), 32)
    turned[pl.ds(beside, 8), :] = part[2 * HEAD + 32 : 2 * HEAD + 40]
    turned[pl.ds(pl.multiple_of(beside + 8, 8), 8), :] = jnp.broadcast_to(squares, (8, SEQS))
    rows, rows_in = s["rows"], s["rows_in"]
    rows[...] = turned[...].T.astype(BF16).reshape(NKV, ROWS, WIDE)

    row_copies = Copies(wire, rows.at[0 : NKV - 1])
    row_copies.arrival(0)

    @pl.loop(1, NKV)
    def _(d):
        peer = lax.rem(kv + d, NKV)
        row_copies.send(rows.at[peer], rows_in.at[kv], peer, tp)

    rows_in[kv] = rows[kv]
    wire.settle((row_copies,))
    wait_down(sets["next_down"], b["down_parts"], b["down_t"])
    staging["state"].wait()
    row_copies.arrived(rows_in.at[0 : NKV - 1])
    mixed, change = state_step(
        s,
        folded,
        conv_weight,
        step_bias,
        log_decay_rate,
        group_gain,
        conv_next,
        s["state"],
        lambda: staging["conv"].wait(),
    )

    mixed_all = s["mixed_all"]
    mixed_all[z, x] = mixed
    own = mixed_all.at[z, x]
    to_z = Copies(wire, mixed_all.at[0 : NZ - 1, 0])
    to_x = Copies(wire, mixed_all.at[0 : NZ - 2])
    for d in plain.near:
        to_z.send(own, own, plain.kv_at(plain.ahead(d), x), tp, d)
    to_x.to_h(plain, lambda peer: own, own)
    sets["second"].append(send_gate_up(wire, plain, b["gate_t"], b["up_t"], b["both"], 1))
    kept_out[...], drive_out[...], write_out[...] = change
    staging["out_weight"].wait()
    wire.settle((to_z, to_x))
    for d in plain.near:
        block = mixed_all.at[plain.behind(d), x]
        to_z.arrived(block, d)
        to_x.to_h(plain, lambda peer: block, block)
    to_x.arrived(to_x.every)
    part = jnp.dot(mixed_all[...].reshape(SEQS, PER * HEAD), s["out_weight"][...], preferred_element_type=F32)
    out_t, out_in = s["out_t"], s["out_in"]
    out_t[...] = part.T.astype(BF16).reshape(NTP, OWN, SEQS)
    to_tp = Copies(wire, out_in.at[0 : NTP - 1])
    to_tp.to_tp(lambda peer: out_t.at[peer], out_in.at[tp])
    out_in[tp] = out_t[tp]
    wire.settle((to_tp,))
    to_tp.arrived(to_tp.every)
    after = (after.astype(F32) + jnp.sum(out_in[...].astype(F32), axis=0)).astype(BF16)

    def bulk_left():
        for copies in [sets["down"], sets["mix"], sets["next_down"], *sum(sets["first"] + sets["second"], [])]:
            copies.left()

    branch = channel_mixer(
        wire,
        plain,
        after,
        gain_3,
        b,
        lambda: None,
        lambda part: wait_all(sets["second"][part]),
        bulk_left,
        b["down_t"],
    )
    result[...] = (after.astype(F32) + 0.5 * branch).astype(BF16)
    wire.settle()


def finish(stream_in, conv_in, kept, drive, write_vec, state, result, conv_next, state_next, held, done, reads, writes):
    into = [pltpu.make_async_copy(state.at[b], held.at[b], reads.at[b]) for b in range(ROWS)]
    out = [pltpu.make_async_copy(done.at[b], state_next.at[b], writes.at[b]) for b in range(ROWS)]
    for copy in into:
        copy.start()
    kept_t, drive_t = kept[...].T, drive[...].T
    result[...] = stream_in[...]
    conv_next[...] = conv_in[...]
    for b in range(ROWS):
        into[b].wait()
        flat = held[b].reshape(PER * HEAD, STATE)
        new = flat * kept_t[:, b : b + 1] + drive_t[:, b : b + 1] * write_vec[b : b + 1]
        done[b] = new.reshape(PER, HEAD, STATE)
        out[b].start()
    for copy in out:
        copy.wait()


def on_device(
    stream,
    ssm_state,
    conv_state,
    first_gain,
    first_gate,
    first_up,
    first_down,
    mix_gain,
    gate_in,
    value_in,
    write_in,
    read_in,
    step_in,
    conv_weight,
    step_bias,
    log_decay_rate,
    group_gain,
    out_weight,
    last_norm_gain,
    second_gate,
    second_up,
    second_down,
):
    staged = dict(
        a_gate=first_gate,
        a_up=first_up,
        a_down=first_down,
        gate_in=gate_in,
        value_in=value_in,
        write_in=write_in,
        read_in=read_in,
        b_down=second_down,
        b_gate=second_gate,
        b_up=second_up,
        state=ssm_state,
        conv=conv_state[:, :, 0].transpose(1, 0, 2),
        out_weight=out_weight,
    )
    small = (
        stream.T,
        first_gain[None],
        mix_gain[None],
        last_norm_gain[None],
        step_in.T,
        conv_weight,
        step_bias[None],
        log_decay_rate[None],
        group_gain[None],
    )
    whole = pl.BlockSpec(memory_space=pltpu.VMEM)
    channels = PER * HEAD + 2 * STATE
    outs = (
        jax.ShapeDtypeStruct((OWN, SEQS), BF16),
        jax.ShapeDtypeStruct((3, ROWS, channels), BF16),
        jax.ShapeDtypeStruct((ROWS, PER * HEAD), F32),
        jax.ShapeDtypeStruct((ROWS, PER * HEAD), F32),
        jax.ShapeDtypeStruct((ROWS, STATE), F32),
    )
    far = pl.BlockSpec(memory_space=pltpu.MemorySpace.HBM)
    parts = pl.pallas_call(
        layer,
        name="layer",
        out_shape=outs,
        in_specs=[whole] * len(small) + [far] * len(STAGED),
        out_specs=[whole] * len(outs),
        scratch_shapes=[pltpu.VMEM(shape, dtype) for shape, dtype in SCRATCH.values()]
        + [
            pltpu.SemaphoreType.DMA((LEAVE,)),
            pltpu.SemaphoreType.DMA((ARRIVE,)),
            pltpu.SemaphoreType.DMA((len(STAGED),)),
        ],
        compiler_params=pltpu.CompilerParams(
            collective_id=0, has_side_effects=True, vmem_limit_bytes=VMEM_LIMIT
        ),
    )(*small, *(staged[name] for name in STAGED))
    state_shape = jax.ShapeDtypeStruct((ROWS, PER, HEAD, STATE), F32)
    result, conv_next, ssm_next = pl.pallas_call(
        finish,
        name="finish",
        out_shape=(*outs[:2], state_shape),
        in_specs=[whole] * len(outs) + [far],
        out_specs=[whole, whole, far],
        scratch_shapes=[pltpu.VMEM(state_shape.shape, F32)] * 2 + [pltpu.SemaphoreType.DMA((ROWS,))] * 2,
        compiler_params=pltpu.CompilerParams(vmem_limit_bytes=VMEM_LIMIT),
    )(*parts, ssm_state)
    return (result.T, ssm_next, conv_next.transpose(1, 0, 2)[:, :, None])


def solution(mesh):
    placed = (
        P(None, ("kv", "tp")),
        P("kv", "tp", None, None),
        P("kv", None, "tp", None),
        P(("kv", "tp")),
        P("kv", "tp"),
        P("kv", "tp"),
        P("tp", "kv"),
        P(("kv", "tp")),
        P("kv", "tp"),
        P("kv", "tp"),
        P("kv", "tp"),
        P("kv", "tp"),
        P("kv", "tp"),
        P(None, "tp", None),
        P("tp"),
        P("tp"),
        P("tp"),
        P("tp", "kv"),
        P(("kv", "tp")),
        P("kv", "tp"),
        P("kv", "tp"),
        P("tp", "kv"),
    )
    return jax.shard_map(
        on_device,
        mesh=mesh,
        in_specs=placed,
        out_specs=(P(None, ("kv", "tp")), P("kv", "tp", None, None), P("kv", None, "tp", None)),
        check_vma=False,
    )
```

```python
import jax
import jax.numpy as jnp
from jax import lax
from jax.experimental import pallas as pl
from jax.experimental.pallas import tpu as pltpu
from jax.sharding import PartitionSpec as P

MESH = pl.DeviceIdType.MESH
F32, BF16 = jnp.float32, jnp.bfloat16

NZ, NX, NY, NC = 8, 4, 4, 2
NKV, NTP = NZ * NX, NY * NC
SEQS, D, FF = 512, 4096, 11264
OWN = D // (NKV * NTP)
FEAT = OWN * NTP
DEPTH = FEAT * NZ
CUT = FF // NTP // NZ
XS = SEQS // NX
ROWS = SEQS // NKV
HEAD, STATE, PER = 64, 128, 8
MIX = 176
WIDE = 256
PARTS = ((0, 96), (96, 80))
norm_epsilon = 1e-06


class Wire:
    def __init__(self, sends, recvs):
        self.sends, self.recvs, self.pending = sends, recvs, []
        self.next = {False: [0, 0], True: [BULK_LEAVE, BULK_ARRIVE]}
        kv, self.tp = lax.axis_index("kv"), lax.axis_index("tp")
        self.kv = kv
        self.z, self.x = lax.div(kv, NX), lax.rem(kv, NX)
        self.y, self.c = lax.div(self.tp, NC), lax.rem(self.tp, NC)
        self.sibling = self.y * NC + (1 - self.c)

    def along_y(self, d):
        return lax.rem(self.y + d, NY)

    def along_tp(self, d):
        return lax.rem(self.tp + d, NTP)

    def start_over(self):
        self.next[False] = [0, 0]

    def take(self, bulk, kind):
        self.next[bulk][kind] += 1
        return self.next[bulk][kind] - 1

    def settle(self, keep=()):
        for copies in self.pending:
            if copies not in keep:
                copies.left()
        self.pending = [copies for copies in self.pending if copies in keep]


class Copies:
    def __init__(self, wire, every, bulk=False):
        self.wire, self.every, self.bulk, self.keys = wire, every, bulk, {}
        self.sem = wire.sends.at[wire.take(bulk, 0)]
        if not bulk:
            wire.pending.append(self)

    def arrival(self, key):
        if key not in self.keys:
            self.keys[key] = self.wire.take(self.bulk, 1)
        return self.wire.recvs.at[self.keys[key]]

    def _copy(self, src, dst, kv, tp, key):
        return pltpu.make_async_remote_copy(
            src_ref=src,
            dst_ref=dst,
            send_sem=self.sem,
            recv_sem=self.arrival(key),
            device_id=(kv, tp),
            device_id_type=MESH,
        )

    def send(self, src, dst, kv, tp, key=0):
        self._copy(src, dst, kv, tp, key).start()

    def arrived(self, whole, key=0):
        self._copy(whole, whole, self.wire.kv, self.wire.sibling, key).wait_recv()

    def left(self):
        self._copy(self.every, self.every, self.wire.kv, self.wire.sibling, next(iter(self.keys))).wait_send()

    def to_y(self, src, dst, key=0):
        wire = self.wire
        for d in (2, 1, 3):
            peer = wire.along_y(d)
            self.send(src(peer), dst, wire.kv, peer * NC + wire.c, key)

    def to_tp(self, src, dst):
        for d in range(1, NTP):
            peer = self.wire.along_tp(d)
            self.send(src(peer), dst, self.wire.kv, peer)

    def to_g(self, plane, src, dst):
        for d in plane.far:
            peer = plane.ahead(d)
            self.send(src(peer), dst, plane.kv_at(peer, plane.h), self.wire.tp)

    def to_h(self, plane, src, dst, key=0):
        for d in (2, 1, 3):
            peer = lax.rem(plane.h + d, NX)
            self.send(src(peer), dst, plane.kv_at(plane.g, peer), self.wire.tp, key)


class Plane:
    def __init__(self, wire, folded):
        self.folded = folded
        if folded:
            self.g, self.h = wire.x + NX * lax.rem(wire.z, 2), lax.div(wire.z, 2)
            self.near = (1, 3, 4, 5, 7, 2, 6)
        else:
            self.g, self.h = wire.z, wire.x
            self.near = (1, 7, 2, 6, 3, 5, 4)
        self.far = self.near[::-1]

    def kv_at(self, g, h):
        if self.folded:
            if isinstance(g, int) and isinstance(h, int):
                return (2 * h + g // NX) * NX + g % NX
            return (2 * h + lax.div(g, NX)) * NX + lax.rem(g, NX)
        return g * NX + h

    def ahead(self, d):
        if not self.folded:
            return lax.rem(self.g + d, NZ)
        x, pair = lax.rem(self.g, NX), lax.div(self.g, NX)
        return lax.rem(x + d % NX, NX) + NX * lax.rem(pair + d // NX, 2)

    def behind(self, d):
        if not self.folded:
            return lax.rem(self.g + NZ - d, NZ)
        x, pair = lax.rem(self.g, NX), lax.div(self.g, NX)
        return lax.rem(x + NX - d % NX, NX) + NX * lax.rem(pair + d // NX, 2)


def greet(wire):
    barrier = pltpu.get_barrier_semaphore()

    def tell(kv, tp):
        pl.semaphore_signal(barrier, inc=1, device_id=(kv, tp), device_id_type=MESH)

    for d in range(1, NZ):
        tell(lax.rem(wire.z + d, NZ) * NX + wire.x, wire.tp)
    for d in range(1, NX):
        x = lax.rem(wire.x + d, NX)
        tell(wire.z * NX + x, wire.tp)
        tell((wire.z + 1 - 2 * lax.rem(wire.z, 2)) * NX + x, wire.tp)
    for d in range(1, NTP):
        tell(wire.kv, wire.along_tp(d))
    return lambda: pl.semaphore_wait(barrier, NZ - 1 + 2 * (NX - 1) + NTP - 1)


def at_rows(start, size, step):
    return pl.ds(pl.multiple_of(start * step, step), size)


def turn_columns(src, dst):
    for j in range(src.shape[1] // 128):
        dst[j * 128 : (j + 1) * 128, :] = src[:, j * 128 : (j + 1) * 128].T


def send_cut(wire, plane, turned, both, part, second):
    g = plane.g
    lanes = at_rows(g, FEAT, FEAT)
    start, size = PARTS[part]
    at = 2 * start + second * size
    copies = Copies(wire, both.at[at : at + size, 0 : (NZ - 1) * FEAT], True)

    def cut(peer):
        return pl.ds(pl.multiple_of(peer * CUT + start, OWN), size)

    copies.to_g(plane, lambda peer: turned.at[cut(peer), :], both.at[at : at + size, lanes])
    both[at : at + size, lanes] = turned[cut(g), :]
    return copies


class Hooks:
    def after_first_sends(self):
        pass

    def after_forwards(self):
        pass

    def after_sums(self):
        pass

    def wait_weights(self, part):
        pass

    def after_hidden(self):
        pass

    def before_down(self):
        pass


def wait_all(sets):
    for copies in sets:
        copies.arrived(copies.every)


def send_down(wire, plane, down, parts):
    g = plane.g
    copies = Copies(wire, parts.at[0 : NZ - 1], True)
    copies.to_g(plane, lambda peer: down.at[at_rows(peer, CUT, CUT), :], parts.at[g])
    parts[g] = down[at_rows(g, CUT, CUT), :]
    return copies


def wait_down(copies, parts, turned):
    copies.arrived(copies.every)
    for s in range(NZ):
        turned[s] = parts[s].T


def silu(v):
    return v / (1.0 + jnp.exp(-v))


def as_column(row):
    square = jnp.broadcast_to(row, (OWN, OWN))
    same = lax.broadcasted_iota(jnp.int32, (OWN, OWN), 0) == lax.broadcasted_iota(jnp.int32, (OWN, OWN), 1)
    return jnp.sum(jnp.where(same, square, 0.0), axis=1, keepdims=True)


def gather_features(wire, plane, values, gain, feats, sq_g, sq_tp, after_first_sends, after_forwards):
    g, tp, c, sibling = plane.g, wire.tp, wire.c, wire.sibling
    wide = values.astype(F32)
    feats[g, tp] = (wide * as_column(gain[...])).astype(BF16)
    own = feats.at[g, tp]
    to_group = Copies(wire, feats.at[0, 0 : NZ - 1])
    for d in plane.near:
        to_group.send(own, own, plane.kv_at(plane.ahead(d), plane.h), tp, d)
    along = Copies(wire, feats.at[0 : NY - 1])
    across = Copies(wire, feats.at[0:NY])

    def hand_on(d, peer):
        block = feats.at[peer, tp]
        along.to_y(lambda p: block, block, d)
        across.send(block, block, wire.kv, sibling)

    hand_on(0, g)
    sq_g[g] = jnp.sum(wide * wide, axis=0, keepdims=True)
    squares_g = Copies(wire, sq_g.at[0 : NZ - 1])
    squares_g.to_g(plane, lambda peer: sq_g.at[g], sq_g.at[g])
    after_first_sends()
    steps = [(0, g)] + [(d, plane.behind(d)) for d in plane.near]
    for d, peer in steps[1:]:
        to_group.arrived(feats.at[peer, tp], d)
        hand_on(d, peer)
    after_forwards()
    squares_g.arrived(squares_g.every)
    sq_tp[tp] = jnp.sum(sq_g[...], axis=0)
    squares_tp = Copies(wire, sq_tp.at[0 : NTP - 1])
    squares_tp.to_tp(lambda peer: sq_tp.at[tp], sq_tp.at[tp])
    for d, peer in steps:
        along.arrived(feats.at[peer, 0 : NY - 1], d)
        for e in (1, 3, 2):
            block = feats.at[peer, wire.along_y(NY - e) * NC + c]
            across.send(block, block, wire.kv, sibling)
    squares_tp.arrived(squares_tp.every)
    across.arrived(across.every)
    return jnp.sum(sq_tp[...], axis=0)


def channel_mixer(wire, plane, values, gain, s, hooks, down_t):
    g, h = plane.g, plane.h
    squares = gather_features(
        wire, plane, values, gain, s["feats"], s["sq_g"], s["sq_tp"], hooks.after_first_sends, hooks.after_forwards
    )
    sq_h, sums, sums_h, hidden = s["sq_h"], s["sums"], s["sums_h"], s["hidden"]
    sq_h[h] = squares
    squares_h = Copies(wire, sq_h.at[0 : NX - 1])
    squares_h.to_h(plane, lambda peer: sq_h.at[h], sq_h.at[h])
    gathered = list(wire.pending)
    sums_out = []
    for part, (start, size) in enumerate(PARTS):
        hooks.wait_weights(part)
        rows = slice(2 * start, 2 * (start + size))
        sums[rows] = jnp.dot(
            s["both"][rows], s["feats"][...].reshape(DEPTH, SEQS), preferred_element_type=F32
        ).astype(BF16)
        copies = Copies(wire, sums_h.at[0 : NX - 1, rows])
        copies.to_h(plane, lambda peer: sums.at[rows, at_rows(peer, XS, XS)], sums_h.at[h, rows])
        sums_h[h, rows] = sums[rows, at_rows(h, XS, XS)]
        sums_out.append(copies)
    hooks.after_sums()
    squares_h.arrived(squares_h.every)
    s["factor"][...] = lax.rsqrt(jnp.sum(sq_h[...], axis=0) / D + norm_epsilon)
    factor = s["factor"][:, at_rows(h, XS, XS)]
    hidden_out = []
    for (start, size), copies in zip(PARTS, sums_out):
        copies.arrived(copies.every)
        at = 2 * start
        gates = sum(sums_h[p, at : at + size].astype(F32) for p in range(NX)) * factor
        ups = sum(sums_h[p, at + size : at + 2 * size].astype(F32) for p in range(NX)) * factor
        here = hidden.at[start : start + size, at_rows(h, XS, XS)]
        here[...] = (silu(gates) * ups).astype(BF16)
        out = Copies(wire, hidden.at[start : start + size, 0 : SEQS - XS])
        out.to_h(plane, lambda peer: here, here)
        hidden_out.append(out)
    hooks.after_hidden()
    for copies in gathered:
        copies.left()
    wire.pending = [copies for copies in wire.pending if copies not in gathered]
    wait_all(hidden_out)
    hooks.before_down()

    c, y = wire.c, wire.y
    outs, other = s["outs"], s["other"]
    by_y, arrived_y = s["by_y"], s["arrived_y"]
    by_g, arrived_g = s["by_g"], s["arrived_g"]
    order = [(d, plane.ahead(d)) for d in plane.far + (0,)]
    across, along = Copies(wire, other), Copies(wire, by_y.at[0 : NY - 1])
    to_group = Copies(wire, by_g.at[0 : NZ - 1])
    for d, k in order:
        part = jnp.dot(down_t[k], hidden[...], preferred_element_type=F32)
        outs[k] = part.astype(BF16).reshape(NY, NC, OWN, SEQS)
        across.send(outs.at[k, :, 1 - c], other.at[k], wire.kv, wire.sibling, d)
    for d, k in order:
        across.arrived(other.at[k], d)
        by_y[:, k] = (outs[k, :, c].astype(F32) + other[k].astype(F32)).astype(BF16)
        along.to_y(lambda peer: by_y.at[peer, k], arrived_y.at[y, k], d)
        arrived_y[y, k] = by_y[y, k]
    for d, k in order:
        along.arrived(arrived_y.at[0 : NY - 1, k], d)
        by_g[k] = sum(arrived_y[p, k].astype(F32) for p in range(NY)).astype(BF16)
        if d:
            to_group.send(by_g.at[k], arrived_g.at[g], plane.kv_at(k, h), wire.tp)
    arrived_g[g] = by_g[g]
    wire.settle((to_group,))
    to_group.arrived(to_group.every)
    return jnp.sum(arrived_g[...].astype(F32), axis=0)


def ff_scratch(name):
    return {
        name + key: value
        for key, value in dict(
            feats=((NZ, NTP, OWN, SEQS), BF16),
            sq_g=((NZ, 1, SEQS), F32),
            sq_tp=((NTP, 1, SEQS), F32),
            sq_h=((NX, 1, SEQS), F32),
            factor=((1, SEQS), F32),
            gate=((FEAT, NZ * CUT), BF16),
            up=((FEAT, NZ * CUT), BF16),
            down=((NZ * CUT, FEAT), BF16),
            gate_t=((NZ * CUT, FEAT), BF16),
            up_t=((NZ * CUT, FEAT), BF16),
            both=((2 * CUT, DEPTH), BF16),
            down_parts=((NZ, CUT, FEAT), BF16),
            down_t=((NZ, FEAT, CUT), BF16),
            sums=((2 * CUT, SEQS), BF16),
            sums_h=((NX, 2 * CUT, XS), BF16),
            hidden=((CUT, SEQS), BF16),
            outs=((NZ, NY, NC, OWN, SEQS), BF16),
            other=((NZ, NY, OWN, SEQS), BF16),
            by_y=((NY, NZ, OWN, SEQS), BF16),
            arrived_y=((NY, NZ, OWN, SEQS), BF16),
            by_g=((NZ, OWN, SEQS), BF16),
            arrived_g=((NZ, OWN, SEQS), BF16),
        ).items()
    }


SCRATCH = dict(
    ff_scratch("a_"),
    **ff_scratch("b_"),
    gate_in=((FEAT, PER * HEAD), BF16),
    value_in=((FEAT, PER * HEAD), BF16),
    write_in=((FEAT, STATE), BF16),
    read_in=((FEAT, STATE), BF16),
    out_weight=((PER * HEAD, FEAT), BF16),
    state=((ROWS, PER, HEAD, STATE), F32),
    conv=((3, ROWS, PER * HEAD + 2 * STATE), BF16),
    conv_next=((3, ROWS, PER * HEAD + 2 * STATE), BF16),
    mix_t=((NZ, MIX, FEAT), BF16),
    mix_in=((MIX, DEPTH), BF16),
    mix_feats=((NZ, NTP, OWN, SEQS), BF16),
    mix_sq_g=((NZ, 1, SEQS), F32),
    mix_sq_tp=((NTP, 1, SEQS), F32),
    turned=((WIDE, SEQS), F32),
    rows=((NKV, ROWS, WIDE), BF16),
    rows_in=((NKV, ROWS, WIDE), BF16),
    mixed_all=((NZ, NX, ROWS, PER * HEAD), BF16),
    out_t=((NTP, OWN, SEQS), BF16),
    out_in=((NTP, OWN, SEQS), BF16),
)
STAGED = (
    "a_gate",
    "a_up",
    "a_down",
    "gate_in",
    "value_in",
    "write_in",
    "read_in",
    "b_down",
    "b_gate",
    "b_up",
    "state",
    "conv",
    "out_weight",
)
BULK_LEAVE, BULK_ARRIVE = 22, 68
LEAVE, ARRIVE = BULK_LEAVE + 11, BULK_ARRIVE + 11
PIECES = 4
VMEM_LIMIT = 58 * 1024 * 1024


def part_of(scratch, name):
    return {key[len(name) :]: ref for key, ref in scratch.items() if key.startswith(name)}


def turn_mixer(s, step_in):
    mix_t = s["mix_t"]
    for j in range(PER * HEAD // 128):
        for ref, at in ((s["gate_in"], 0), (s["value_in"], HEAD)):
            tile = ref[:, j * 128 : (j + 1) * 128].T
            mix_t[2 * j, at : at + HEAD] = tile[:HEAD]
            mix_t[2 * j + 1, at : at + HEAD] = tile[HEAD:]
    for ref, base in ((s["write_in"], 0), (s["read_in"], 4)):
        tile = ref[...].T
        for j in range(4):
            mix_t[base + j, 2 * HEAD : 2 * HEAD + 32] = tile[32 * j : 32 * (j + 1)]
    steps = jnp.concatenate([step_in[...].astype(F32), jnp.zeros((8, FEAT), F32)], axis=0).astype(BF16)
    for j in range(NZ):
        mix_t[j, 2 * HEAD + 32 : MIX] = steps


def state_step(s, plane, conv_weight, step_bias, log_decay_rate, group_gain, conv_next, state, ready):
    rows_in = s["rows_in"]
    parts = [sum(rows_in[plane.kv_at(k, p)].astype(F32) for p in range(NX)) for k in range(NZ)]
    factor = lax.rsqrt(parts[3][:, 2 * HEAD + 8 : 2 * HEAD + 9] / D + norm_epsilon)
    parts = [(part * factor).astype(BF16).astype(F32) for part in parts]
    lane = lax.broadcasted_iota(jnp.int32, (ROWS, 128), 1)
    low = lane < HEAD
    gates, values, writes, reads = [], [], 0.0, 0.0
    for j in range(PER // 2):
        a, b = parts[2 * j][:, :128], parts[2 * j + 1][:, :128]
        gates.append(jnp.where(low, a, pltpu.roll(b, HEAD, 1)))
        values.append(jnp.where(low, pltpu.roll(a, HEAD, 1), b))
    for k in range(4):
        here = lane // 32 == k
        writes = writes + jnp.where(here, parts[k][:, 128:], 0.0)
        reads = reads + jnp.where(here, parts[4 + k][:, 128:], 0.0)
    gate = jnp.concatenate(gates, axis=1)
    fresh = jnp.concatenate([*values, writes, reads], axis=1)
    ready()
    conv = s["conv"]
    conv_next[0] = conv[1]
    conv_next[1] = conv[2]
    conv_next[2] = fresh.astype(BF16)
    total = fresh * conv_weight[3]
    for t in range(3):
        total = total + conv[t].astype(F32) * conv_weight[t]
    activated = silu(total)
    inputs = activated[:, : PER * HEAD]
    write_vec = activated[:, PER * HEAD : PER * HEAD + STATE]
    read_vec = activated[:, PER * HEAD + STATE :]
    raw_step = parts[3][:, 128 : 128 + PER] + step_bias[...]
    step_size = jnp.maximum(raw_step, 0.0) + jnp.log1p(jnp.exp(-jnp.abs(raw_step)))
    decay = jnp.exp(-step_size * jnp.exp(log_decay_rate[...]))

    def over_heads(v):
        return jnp.concatenate(
            [jnp.where(low, v[:, 2 * j : 2 * j + 1], v[:, 2 * j + 1 : 2 * j + 2]) for j in range(PER // 2)],
            axis=1,
        )

    drive, kept = over_heads(step_size) * inputs, over_heads(decay)
    row = lax.broadcasted_iota(jnp.int32, (ROWS, STATE), 0)
    carried = 0.0
    for b in range(ROWS):
        one = jnp.where(row == b, read_vec, 0.0).astype(BF16)
        flat = state[b].reshape(PER * HEAD, STATE).astype(BF16)
        carried = carried + lax.dot_general(one, flat, (((1,), (1,)), ((), ())), preferred_element_type=F32)
    readout = kept * carried + drive * jnp.sum(write_vec * read_vec, axis=1, keepdims=True)
    gated = readout * silu(gate)
    scale = lax.rsqrt(jnp.mean(gated * gated, axis=1, keepdims=True) + norm_epsilon)
    return (gated * scale * group_gain[...]).astype(BF16), (kept, drive, write_vec)


def update_state(state, kept, drive, write_vec):
    kept, drive = kept.T, drive.T
    for b in range(ROWS):
        flat = state[b].reshape(PER * HEAD, STATE)
        new = flat * kept[:, b : b + 1] + drive[:, b : b + 1] * write_vec[b : b + 1]
        state[b] = new.reshape(PER, HEAD, STATE)


def layer(*refs):
    (stream, gain_1, gain_2, gain_3, step_in, conv_weight, step_bias, log_decay_rate, group_gain) = refs[:9]
    held = dict(zip(STAGED, refs[9 : 9 + len(STAGED)]))
    refs = refs[9 + len(STAGED) :]
    result, conv_next, state_next = refs[:3]
    refs = refs[3:]
    s = dict(zip(SCRATCH, refs))
    sends, recvs, stage_sems, early_sems = refs[len(SCRATCH) :]
    wire = Wire(sends, recvs)
    plain, folded = Plane(wire, False), Plane(wire, True)
    z, x, kv, tp = wire.z, wire.x, wire.kv, wire.tp
    wait_greeting = greet(wire)

    staging = {
        name: pltpu.make_async_copy(held[name], s[name], stage_sems.at[i]) for i, name in enumerate(STAGED)
    }
    for copy in staging.values():
        copy.start()
    a, b = part_of(s, "a_"), part_of(s, "b_")
    staging["a_gate"].wait()
    turn_columns(a["gate"], a["gate_t"])
    staging["a_up"].wait()
    turn_columns(a["up"], a["up_t"])
    wait_greeting()
    sets = {}
    early = [
        pltpu.make_async_copy(s["conv_next"], conv_next, early_sems.at[0]),
        pltpu.make_async_copy(s["state"], state_next, early_sems.at[1]),
    ]

    class First(Hooks):
        def after_first_sends(self):
            sets["first"] = {0: [send_cut(wire, folded, a["gate_t"], a["both"], 0, 0)]}
            sets["first"][0].append(send_cut(wire, folded, a["up_t"], a["both"], 0, 1))

        def after_forwards(self):
            sets["first"][1] = [send_cut(wire, folded, a["gate_t"], a["both"], 1, 0)]
            sets["first"][1].append(send_cut(wire, folded, a["up_t"], a["both"], 1, 1))

        def after_sums(self):
            staging["a_down"].wait()
            sets["down"] = send_down(wire, folded, a["down"], a["down_parts"])

        def wait_weights(self, part):
            wait_all(sets["first"][part])

        def after_hidden(self):
            for name in ("gate_in", "value_in", "write_in", "read_in"):
                staging[name].wait()
            turn_mixer(s, step_in)
            s["mix_in"][:, at_rows(folded.g, FEAT, FEAT)] = s["mix_t"][folded.g]
            wait_down(sets["down"], a["down_parts"], a["down_t"])

        def before_down(self):
            lanes = at_rows(folded.g, FEAT, FEAT)
            sets["mix"] = Copies(wire, s["mix_in"].at[:, 0 : (NZ - 1) * FEAT], True)
            sets["mix"].to_g(folded, lambda peer: s["mix_t"].at[peer], s["mix_in"].at[:, lanes])

    branch = channel_mixer(wire, folded, stream[...], gain_1, a, First(), a["down_t"])
    after = (stream[...].astype(F32) + 0.5 * branch).astype(BF16)

    def next_down():
        staging["b_down"].wait()
        sets["next_down"] = send_down(wire, plain, b["down"], b["down_parts"])
        staging["b_gate"].wait()
        turn_columns(b["gate"], b["gate_t"])
        staging["b_up"].wait()
        turn_columns(b["up"], b["up_t"])

    squares = gather_features(
        wire, folded, after, gain_2, s["mix_feats"], s["mix_sq_g"], s["mix_sq_tp"], next_down, lambda: None
    )
    wait_all([sets["mix"]])
    part = jnp.dot(s["mix_in"][...], s["mix_feats"][...].reshape(DEPTH, SEQS), preferred_element_type=F32)
    turned = s["turned"]
    turned[2 * HEAD :, :] = jnp.zeros((WIDE - 2 * HEAD, SEQS), F32)
    turned[: 2 * HEAD, :] = part[: 2 * HEAD]
    quarter = lax.rem(folded.g, 4)
    turned[pl.ds(pl.multiple_of(128 + 32 * quarter, 32), 32), :] = part[2 * HEAD : 2 * HEAD + 32]
    beside = pl.multiple_of(128 + 32 * lax.rem(folded.g + 1, 4), 32)
    turned[pl.ds(beside, 8), :] = part[2 * HEAD + 32 : 2 * HEAD + 40]
    turned[pl.ds(pl.multiple_of(beside + 8, 8), 8), :] = jnp.broadcast_to(squares, (8, SEQS))
    rows, rows_in = s["rows"], s["rows_in"]
    rows[...] = turned[...].T.astype(BF16).reshape(NKV, ROWS, WIDE)

    row_copies = Copies(wire, rows.at[0 : NKV - 1])
    row_copies.arrival(0)

    @pl.loop(1, NKV)
    def _(d):
        peer = lax.rem(kv + d, NKV)
        row_copies.send(rows.at[peer], rows_in.at[kv], peer, tp)

    sets["second"] = {0: [send_cut(wire, plain, b["gate_t"], b["both"], 0, 0)]}
    rows_in[kv] = rows[kv]
    wire.settle((row_copies,))
    wait_down(sets["next_down"], b["down_parts"], b["down_t"])
    staging["state"].wait()
    row_copies.arrived(rows_in.at[0 : NKV - 1])
    mixed, change = state_step(
        s,
        folded,
        conv_weight,
        step_bias,
        log_decay_rate,
        group_gain,
        s["conv_next"],
        s["state"],
        lambda: staging["conv"].wait(),
    )

    mixed_all = s["mixed_all"]
    mixed_all[z, x] = mixed
    own = mixed_all.at[z, x]
    to_z = Copies(wire, mixed_all.at[0 : NZ - 1, 0])
    to_x = Copies(wire, mixed_all.at[0 : NZ - 2])
    for d in plain.near:
        to_z.send(own, own, plain.kv_at(plain.ahead(d), x), tp, d)
    to_x.to_h(plain, lambda peer: own, own)
    early[0].start()
    staging["out_weight"].wait()
    wire.settle((to_z, to_x))
    for d in plain.near:
        block = mixed_all.at[plain.behind(d), x]
        to_z.arrived(block, d)
        to_x.to_h(plain, lambda peer: block, block)
    sets["second"][0].append(send_cut(wire, plain, b["up_t"], b["both"], 0, 1))
    sets["second"][1] = [send_cut(wire, plain, b["gate_t"], b["both"], 1, 0)]
    sets["second"][1].append(send_cut(wire, plain, b["up_t"], b["both"], 1, 1))
    to_x.arrived(to_x.every)
    part = jnp.dot(mixed_all[...].reshape(SEQS, PER * HEAD), s["out_weight"][...], preferred_element_type=F32)
    out_t, out_in = s["out_t"], s["out_in"]
    out_t[...] = part.T.astype(BF16).reshape(NTP, OWN, SEQS)
    to_tp = Copies(wire, out_in.at[0 : NTP - 1])
    to_tp.to_tp(lambda peer: out_t.at[peer], out_in.at[tp])
    out_in[tp] = out_t[tp]
    wire.settle((to_tp,))
    update_state(s["state"], *change)
    early[1].start()
    to_tp.arrived(to_tp.every)
    after = (after.astype(F32) + jnp.sum(out_in[...].astype(F32), axis=0)).astype(BF16)

    assert wire.next[False] == [BULK_LEAVE, BULK_ARRIVE], wire.next

    class Second(Hooks):
        def wait_weights(self, part):
            wait_all(sets["second"][part])

        def after_hidden(self):
            gates_ups = [copies for part in (0, 1) for name in ("first", "second") for copies in sets[name][part]]
            for copies in [sets["down"], sets["mix"], sets["next_down"], *gates_ups]:
                copies.left()
            for copy in early:
                copy.wait()

    wire.start_over()
    branch = channel_mixer(wire, plain, after, gain_3, b, Second(), b["down_t"])
    assert wire.next[True] == [LEAVE, ARRIVE]
    result[...] = (after.astype(F32) + 0.5 * branch).astype(BF16)
    wire.settle()


def finish(*refs):
    far_in, far_out, near = refs[:3], refs[3:6], refs[6:9]
    reads, writes = refs[9:]
    piece = ROWS // PIECES
    pairs = [(far_in[i], near[i], far_out[i]) for i in (0, 1)]
    for i in range(PIECES):
        at = pl.ds(i * piece, piece)
        pairs.append(tuple(ref.at[at] for ref in (far_in[2], near[2], far_out[2])))
    into = [pltpu.make_async_copy(a, b, reads.at[i]) for i, (a, b, _) in enumerate(pairs)]
    out = [pltpu.make_async_copy(b, c, writes.at[i]) for i, (_, b, c) in enumerate(pairs)]
    for copy in into:
        copy.start()
    for first, second in zip(into, out):
        first.wait()
        second.start()
    for copy in out:
        copy.wait()


def on_device(
    stream,
    ssm_state,
    conv_state,
    first_gain,
    first_gate,
    first_up,
    first_down,
    mix_gain,
    gate_in,
    value_in,
    write_in,
    read_in,
    step_in,
    conv_weight,
    step_bias,
    log_decay_rate,
    group_gain,
    out_weight,
    last_norm_gain,
    second_gate,
    second_up,
    second_down,
):
    staged = dict(
        a_gate=first_gate,
        a_up=first_up,
        a_down=first_down,
        gate_in=gate_in,
        value_in=value_in,
        write_in=write_in,
        read_in=read_in,
        b_down=second_down,
        b_gate=second_gate,
        b_up=second_up,
        state=ssm_state,
        conv=conv_state[:, :, 0].transpose(1, 0, 2),
        out_weight=out_weight,
    )
    small = (
        stream.T,
        first_gain[None],
        mix_gain[None],
        last_norm_gain[None],
        step_in.T,
        conv_weight,
        step_bias[None],
        log_decay_rate[None],
        group_gain[None],
    )
    whole = pl.BlockSpec(memory_space=pltpu.VMEM)
    channels = PER * HEAD + 2 * STATE
    channels = PER * HEAD + 2 * STATE
    outs = (
        jax.ShapeDtypeStruct((OWN, SEQS), BF16),
        jax.ShapeDtypeStruct((3, ROWS, channels), BF16),
        jax.ShapeDtypeStruct((ROWS, PER, HEAD, STATE), F32),
    )
    far = pl.BlockSpec(memory_space=pltpu.MemorySpace.HBM)
    parts = pl.pallas_call(
        layer,
        name="layer",
        out_shape=outs,
        in_specs=[whole] * len(small) + [far] * len(STAGED),
        out_specs=[whole] + [far] * (len(outs) - 1),
        scratch_shapes=[pltpu.VMEM(shape, dtype) for shape, dtype in SCRATCH.values()]
        + [
            pltpu.SemaphoreType.DMA((LEAVE,)),
            pltpu.SemaphoreType.DMA((ARRIVE,)),
            pltpu.SemaphoreType.DMA((len(STAGED),)),
            pltpu.SemaphoreType.DMA((len(outs) - 1,)),
        ],
        compiler_params=pltpu.CompilerParams(
            collective_id=0, has_side_effects=True, vmem_limit_bytes=VMEM_LIMIT
        ),
    )(*small, *(staged[name] for name in STAGED))
    result, conv_next, ssm_next = pl.pallas_call(
        finish,
        name="finish",
        out_shape=outs,
        in_specs=[far] * len(outs),
        out_specs=[far] * len(outs),
        scratch_shapes=[pltpu.VMEM(out.shape, out.dtype) for out in outs]
        + [pltpu.SemaphoreType.DMA((PIECES + 2,))] * 2,
        compiler_params=pltpu.CompilerParams(vmem_limit_bytes=VMEM_LIMIT),
    )(*parts)
    return (result.T, ssm_next, conv_next.transpose(1, 0, 2)[:, :, None])


def solution(mesh):
    placed = (
        P(None, ("kv", "tp")),
        P("kv", "tp", None, None),
        P("kv", None, "tp", None),
        P(("kv", "tp")),
        P("kv", "tp"),
        P("kv", "tp"),
        P("tp", "kv"),
        P(("kv", "tp")),
        P("kv", "tp"),
        P("kv", "tp"),
        P("kv", "tp"),
        P("kv", "tp"),
        P("kv", "tp"),
        P(None, "tp", None),
        P("tp"),
        P("tp"),
        P("tp"),
        P("tp", "kv"),
        P(("kv", "tp")),
        P("kv", "tp"),
        P("kv", "tp"),
        P("tp", "kv"),
    )
    return jax.shard_map(
        on_device,
        mesh=mesh,
        in_specs=placed,
        out_specs=(P(None, ("kv", "tp")), P("kv", "tp", None, None), P("kv", None, "tp", None)),
        check_vma=False,
    )
```

```python
import jax
import jax.numpy as jnp
from jax import lax
from jax.experimental import pallas as pl
from jax.experimental.pallas import tpu as pltpu
from jax.sharding import PartitionSpec as P

MESH = pl.DeviceIdType.MESH
F32, BF16 = jnp.float32, jnp.bfloat16

NZ, NX, NY, NC = 8, 4, 4, 2
NKV, NTP = NZ * NX, NY * NC
SEQS, D, FF = 512, 4096, 11264
OWN = D // (NKV * NTP)
FEAT = OWN * NTP
DEPTH = FEAT * NZ
CUT = FF // NTP // NZ
XS = SEQS // NX
ROWS = SEQS // NKV
HEAD, STATE, PER = 64, 128, 8
MIX = 176
WIDE = 256
PARTS = ((0, 96), (96, 80))
norm_epsilon = 1e-06


class Wire:
    def __init__(self, sends, recvs):
        self.sends, self.recvs, self.pending = sends, recvs, []
        self.next = {False: [0, 0], True: [BULK_LEAVE, BULK_ARRIVE]}
        kv, self.tp = lax.axis_index("kv"), lax.axis_index("tp")
        self.kv = kv
        self.z, self.x = lax.div(kv, NX), lax.rem(kv, NX)
        self.y, self.c = lax.div(self.tp, NC), lax.rem(self.tp, NC)
        self.sibling = self.y * NC + (1 - self.c)

    def along_y(self, d):
        return lax.rem(self.y + d, NY)

    def along_tp(self, d):
        return lax.rem(self.tp + d, NTP)

    def start_over(self):
        self.next[False] = [0, 0]

    def take(self, bulk, kind):
        self.next[bulk][kind] += 1
        return self.next[bulk][kind] - 1

    def settle(self, keep=()):
        for copies in self.pending:
            if copies not in keep:
                copies.left()
        self.pending = [copies for copies in self.pending if copies in keep]


class Copies:
    def __init__(self, wire, every, bulk=False):
        self.wire, self.every, self.bulk, self.keys = wire, every, bulk, {}
        self.sem = wire.sends.at[wire.take(bulk, 0)]
        if not bulk:
            wire.pending.append(self)

    def arrival(self, key):
        if key not in self.keys:
            self.keys[key] = self.wire.take(self.bulk, 1)
        return self.wire.recvs.at[self.keys[key]]

    def _copy(self, src, dst, kv, tp, key):
        return pltpu.make_async_remote_copy(
            src_ref=src,
            dst_ref=dst,
            send_sem=self.sem,
            recv_sem=self.arrival(key),
            device_id=(kv, tp),
            device_id_type=MESH,
        )

    def send(self, src, dst, kv, tp, key=0):
        self._copy(src, dst, kv, tp, key).start()

    def arrived(self, whole, key=0):
        self._copy(whole, whole, self.wire.kv, self.wire.sibling, key).wait_recv()

    def left(self):
        self._copy(self.every, self.every, self.wire.kv, self.wire.sibling, next(iter(self.keys))).wait_send()

    def to_y(self, src, dst, key=0):
        wire = self.wire
        for d in (2, 1, 3):
            peer = wire.along_y(d)
            self.send(src(peer), dst, wire.kv, peer * NC + wire.c, key)

    def to_tp(self, src, dst):
        for d in range(1, NTP):
            peer = self.wire.along_tp(d)
            self.send(src(peer), dst, self.wire.kv, peer)

    def to_g(self, plane, src, dst):
        for d in plane.far:
            peer = plane.ahead(d)
            self.send(src(peer), dst, plane.kv_at(peer, plane.h), self.wire.tp)

    def to_h(self, plane, src, dst, key=0):
        for d in (2, 1, 3):
            peer = lax.rem(plane.h + d, NX)
            self.send(src(peer), dst, plane.kv_at(plane.g, peer), self.wire.tp, key)


class Plane:
    def __init__(self, wire, folded):
        self.folded = folded
        if folded:
            self.g, self.h = wire.x + NX * lax.rem(wire.z, 2), lax.div(wire.z, 2)
            self.near = (1, 3, 4, 5, 7, 2, 6)
        else:
            self.g, self.h = wire.z, wire.x
            self.near = (1, 7, 2, 6, 3, 5, 4)
        self.far = self.near[::-1]

    def kv_at(self, g, h):
        if self.folded:
            if isinstance(g, int) and isinstance(h, int):
                return (2 * h + g // NX) * NX + g % NX
            return (2 * h + lax.div(g, NX)) * NX + lax.rem(g, NX)
        return g * NX + h

    def ahead(self, d):
        if not self.folded:
            return lax.rem(self.g + d, NZ)
        x, pair = lax.rem(self.g, NX), lax.div(self.g, NX)
        return lax.rem(x + d % NX, NX) + NX * lax.rem(pair + d // NX, 2)

    def behind(self, d):
        if not self.folded:
            return lax.rem(self.g + NZ - d, NZ)
        x, pair = lax.rem(self.g, NX), lax.div(self.g, NX)
        return lax.rem(x + NX - d % NX, NX) + NX * lax.rem(pair + d // NX, 2)


def greet(wire):
    barrier = pltpu.get_barrier_semaphore()

    def tell(kv, tp):
        pl.semaphore_signal(barrier, inc=1, device_id=(kv, tp), device_id_type=MESH)

    for d in range(1, NZ):
        tell(lax.rem(wire.z + d, NZ) * NX + wire.x, wire.tp)
    for d in range(1, NX):
        x = lax.rem(wire.x + d, NX)
        tell(wire.z * NX + x, wire.tp)
        tell((wire.z + 1 - 2 * lax.rem(wire.z, 2)) * NX + x, wire.tp)
    for d in range(1, NTP):
        tell(wire.kv, wire.along_tp(d))
    return lambda: pl.semaphore_wait(barrier, NZ - 1 + 2 * (NX - 1) + NTP - 1)


def at_rows(start, size, step):
    return pl.ds(pl.multiple_of(start * step, step), size)


def turn_columns(src, dst):
    for j in range(src.shape[1] // 128):
        dst[j * 128 : (j + 1) * 128, :] = src[:, j * 128 : (j + 1) * 128].T


def send_cut(wire, plane, turned, both, part, second):
    g = plane.g
    lanes = at_rows(g, FEAT, FEAT)
    start, size = PARTS[part]
    at = 2 * start + second * size
    copies = Copies(wire, both.at[at : at + size, 0 : (NZ - 1) * FEAT], True)

    def cut(peer):
        return pl.ds(pl.multiple_of(peer * CUT + start, OWN), size)

    copies.to_g(plane, lambda peer: turned.at[cut(peer), :], both.at[at : at + size, lanes])
    both[at : at + size, lanes] = turned[cut(g), :]
    return copies


class Hooks:
    def after_first_sends(self):
        pass

    def after_forwards(self):
        pass

    def after_sums(self):
        pass

    def wait_weights(self, part):
        pass

    def after_hidden(self):
        pass

    def before_down(self):
        pass


def wait_all(sets):
    for copies in sets:
        copies.arrived(copies.every)


def send_down(wire, plane, down, parts):
    g = plane.g
    copies = Copies(wire, parts.at[0 : NZ - 1], True)
    copies.to_g(plane, lambda peer: down.at[at_rows(peer, CUT, CUT), :], parts.at[g])
    parts[g] = down[at_rows(g, CUT, CUT), :]
    return copies


def wait_down(copies, parts, turned):
    copies.arrived(copies.every)
    for s in range(NZ):
        turned[s] = parts[s].T


def silu(v):
    return v / (1.0 + jnp.exp(-v))


def as_column(row):
    square = jnp.broadcast_to(row, (OWN, OWN))
    same = lax.broadcasted_iota(jnp.int32, (OWN, OWN), 0) == lax.broadcasted_iota(jnp.int32, (OWN, OWN), 1)
    return jnp.sum(jnp.where(same, square, 0.0), axis=1, keepdims=True)


def gather_features(wire, plane, values, gain, feats, sq_g, sq_tp, after_first_sends, after_forwards):
    g, tp, c, sibling = plane.g, wire.tp, wire.c, wire.sibling
    wide = values.astype(F32)
    feats[g, tp] = (wide * as_column(gain[...])).astype(BF16)
    own = feats.at[g, tp]
    to_group = Copies(wire, feats.at[0, 0 : NZ - 1])
    along = Copies(wire, feats.at[0 : NY - 1])
    across = Copies(wire, feats.at[0:NY])

    def hand_on(d, peer):
        block = feats.at[peer, tp]
        along.to_y(lambda p: block, block, d)
        across.send(block, block, wire.kv, sibling)

    hand_on(0, g)
    for d in plane.near:
        to_group.send(own, own, plane.kv_at(plane.ahead(d), plane.h), tp, d)
    sq_g[g] = jnp.sum(wide * wide, axis=0, keepdims=True)
    squares_g = Copies(wire, sq_g.at[0 : NZ - 1])
    squares_g.to_g(plane, lambda peer: sq_g.at[g], sq_g.at[g])
    after_first_sends()
    steps = [(0, g)] + [(d, plane.behind(d)) for d in plane.near]
    for d, peer in steps[1:]:
        to_group.arrived(feats.at[peer, tp], d)
        hand_on(d, peer)
    after_forwards()
    squares_g.arrived(squares_g.every)
    sq_tp[tp] = jnp.sum(sq_g[...], axis=0)
    squares_tp = Copies(wire, sq_tp.at[0 : NTP - 1])
    squares_tp.to_tp(lambda peer: sq_tp.at[tp], sq_tp.at[tp])
    for d, peer in steps:
        along.arrived(feats.at[peer, 0 : NY - 1], d)
        for e in (1, 3, 2):
            block = feats.at[peer, wire.along_y(NY - e) * NC + c]
            across.send(block, block, wire.kv, sibling)
    squares_tp.arrived(squares_tp.every)
    across.arrived(across.every)
    return jnp.sum(sq_tp[...], axis=0)


def channel_mixer(wire, plane, values, gain, s, hooks, down_t):
    g, h = plane.g, plane.h
    squares = gather_features(
        wire, plane, values, gain, s["feats"], s["sq_g"], s["sq_tp"], hooks.after_first_sends, hooks.after_forwards
    )
    sq_h, sums, sums_h, hidden = s["sq_h"], s["sums"], s["sums_h"], s["hidden"]
    sq_h[h] = squares
    squares_h = Copies(wire, sq_h.at[0 : NX - 1])
    squares_h.to_h(plane, lambda peer: sq_h.at[h], sq_h.at[h])
    gathered = list(wire.pending)
    sums_out = []
    for part, (start, size) in enumerate(PARTS):
        hooks.wait_weights(part)
        rows = slice(2 * start, 2 * (start + size))
        sums[rows] = jnp.dot(
            s["both"][rows], s["feats"][...].reshape(DEPTH, SEQS), preferred_element_type=F32
        ).astype(BF16)
        copies = Copies(wire, sums_h.at[0 : NX - 1, rows])
        copies.to_h(plane, lambda peer: sums.at[rows, at_rows(peer, XS, XS)], sums_h.at[h, rows])
        sums_h[h, rows] = sums[rows, at_rows(h, XS, XS)]
        sums_out.append(copies)
    hooks.after_sums()
    squares_h.arrived(squares_h.every)
    s["factor"][...] = lax.rsqrt(jnp.sum(sq_h[...], axis=0) / D + norm_epsilon)
    factor = s["factor"][:, at_rows(h, XS, XS)]
    hidden_out = []
    for (start, size), copies in zip(PARTS, sums_out):
        copies.arrived(copies.every)
        at = 2 * start
        gates = sum(sums_h[p, at : at + size].astype(F32) for p in range(NX)) * factor
        ups = sum(sums_h[p, at + size : at + 2 * size].astype(F32) for p in range(NX)) * factor
        here = hidden.at[start : start + size, at_rows(h, XS, XS)]
        here[...] = (silu(gates) * ups).astype(BF16)
        out = Copies(wire, hidden.at[start : start + size, 0 : SEQS - XS])
        out.to_h(plane, lambda peer: here, here)
        hidden_out.append(out)
    hooks.after_hidden()
    for copies in gathered:
        copies.left()
    wire.pending = [copies for copies in wire.pending if copies not in gathered]
    wait_all(hidden_out)
    hooks.before_down()

    c, y = wire.c, wire.y
    outs, other = s["outs"], s["other"]
    by_y, arrived_y = s["by_y"], s["arrived_y"]
    by_g, arrived_g = s["by_g"], s["arrived_g"]
    order = [(d, plane.ahead(d)) for d in plane.far + (0,)]
    across, along = Copies(wire, other), Copies(wire, by_y.at[0 : NY - 1])
    to_group = Copies(wire, by_g.at[0 : NZ - 1])
    for d, k in order:
        part = jnp.dot(down_t[k], hidden[...], preferred_element_type=F32)
        outs[k] = part.astype(BF16).reshape(NY, NC, OWN, SEQS)
        across.send(outs.at[k, :, 1 - c], other.at[k], wire.kv, wire.sibling, d)
    for d, k in order:
        across.arrived(other.at[k], d)
        by_y[:, k] = (outs[k, :, c].astype(F32) + other[k].astype(F32)).astype(BF16)
        along.to_y(lambda peer: by_y.at[peer, k], arrived_y.at[y, k], d)
        arrived_y[y, k] = by_y[y, k]
    for d, k in order:
        along.arrived(arrived_y.at[0 : NY - 1, k], d)
        by_g[k] = sum(arrived_y[p, k].astype(F32) for p in range(NY)).astype(BF16)
        if d:
            to_group.send(by_g.at[k], arrived_g.at[g], plane.kv_at(k, h), wire.tp)
    arrived_g[g] = by_g[g]
    wire.settle((to_group,))
    to_group.arrived(to_group.every)
    return jnp.sum(arrived_g[...].astype(F32), axis=0)


def ff_scratch(name):
    return {
        name + key: value
        for key, value in dict(
            feats=((NZ, NTP, OWN, SEQS), BF16),
            sq_g=((NZ, 1, SEQS), F32),
            sq_tp=((NTP, 1, SEQS), F32),
            sq_h=((NX, 1, SEQS), F32),
            factor=((1, SEQS), F32),
            gate=((FEAT, NZ * CUT), BF16),
            up=((FEAT, NZ * CUT), BF16),
            down=((NZ * CUT, FEAT), BF16),
            gate_t=((NZ * CUT, FEAT), BF16),
            up_t=((NZ * CUT, FEAT), BF16),
            both=((2 * CUT, DEPTH), BF16),
            down_parts=((NZ, CUT, FEAT), BF16),
            down_t=((NZ, FEAT, CUT), BF16),
            sums=((2 * CUT, SEQS), BF16),
            sums_h=((NX, 2 * CUT, XS), BF16),
            hidden=((CUT, SEQS), BF16),
            outs=((NZ, NY, NC, OWN, SEQS), BF16),
            other=((NZ, NY, OWN, SEQS), BF16),
            by_y=((NY, NZ, OWN, SEQS), BF16),
            arrived_y=((NY, NZ, OWN, SEQS), BF16),
            by_g=((NZ, OWN, SEQS), BF16),
            arrived_g=((NZ, OWN, SEQS), BF16),
        ).items()
    }


SCRATCH = dict(
    ff_scratch("a_"),
    **ff_scratch("b_"),
    gate_in=((FEAT, PER * HEAD), BF16),
    value_in=((FEAT, PER * HEAD), BF16),
    write_in=((FEAT, STATE), BF16),
    read_in=((FEAT, STATE), BF16),
    out_weight=((PER * HEAD, FEAT), BF16),
    state=((ROWS, PER, HEAD, STATE), F32),
    conv=((3, ROWS, PER * HEAD + 2 * STATE), BF16),
    conv_next=((3, ROWS, PER * HEAD + 2 * STATE), BF16),
    mix_t=((NZ, MIX, FEAT), BF16),
    mix_in=((MIX, DEPTH), BF16),
    mix_feats=((NZ, NTP, OWN, SEQS), BF16),
    mix_sq_g=((NZ, 1, SEQS), F32),
    mix_sq_tp=((NTP, 1, SEQS), F32),
    turned=((WIDE, SEQS), F32),
    rows=((NKV, ROWS, WIDE), BF16),
    rows_in=((NKV, ROWS, WIDE), BF16),
    mixed_all=((NZ, NX, ROWS, PER * HEAD), BF16),
    out_t=((NTP, OWN, SEQS), BF16),
    out_in=((NTP, OWN, SEQS), BF16),
)
STAGED = (
    "a_gate",
    "a_up",
    "a_down",
    "gate_in",
    "value_in",
    "write_in",
    "read_in",
    "b_down",
    "b_gate",
    "b_up",
    "state",
    "conv",
    "out_weight",
)
BULK_LEAVE, BULK_ARRIVE = 22, 68
LEAVE, ARRIVE = BULK_LEAVE + 11, BULK_ARRIVE + 11
PIECES = 4
VMEM_LIMIT = 58 * 1024 * 1024


def part_of(scratch, name):
    return {key[len(name) :]: ref for key, ref in scratch.items() if key.startswith(name)}


def turn_mixer(s, step_in):
    mix_t = s["mix_t"]
    for j in range(PER * HEAD // 128):
        for ref, at in ((s["gate_in"], 0), (s["value_in"], HEAD)):
            tile = ref[:, j * 128 : (j + 1) * 128].T
            mix_t[2 * j, at : at + HEAD] = tile[:HEAD]
            mix_t[2 * j + 1, at : at + HEAD] = tile[HEAD:]
    for ref, base in ((s["write_in"], 0), (s["read_in"], 4)):
        tile = ref[...].T
        for j in range(4):
            mix_t[base + j, 2 * HEAD : 2 * HEAD + 32] = tile[32 * j : 32 * (j + 1)]
    steps = jnp.concatenate([step_in[...].astype(F32), jnp.zeros((8, FEAT), F32)], axis=0).astype(BF16)
    for j in range(NZ):
        mix_t[j, 2 * HEAD + 32 : MIX] = steps


def state_step(s, plane, conv_weight, step_bias, log_decay_rate, group_gain, conv_next, state, ready):
    rows_in = s["rows_in"]
    parts = [sum(rows_in[plane.kv_at(k, p)].astype(F32) for p in range(NX)) for k in range(NZ)]
    factor = lax.rsqrt(parts[3][:, 2 * HEAD + 8 : 2 * HEAD + 9] / D + norm_epsilon)
    parts = [(part * factor).astype(BF16).astype(F32) for part in parts]
    lane = lax.broadcasted_iota(jnp.int32, (ROWS, 128), 1)
    low = lane < HEAD
    gates, values, writes, reads = [], [], 0.0, 0.0
    for j in range(PER // 2):
        a, b = parts[2 * j][:, :128], parts[2 * j + 1][:, :128]
        gates.append(jnp.where(low, a, pltpu.roll(b, HEAD, 1)))
        values.append(jnp.where(low, pltpu.roll(a, HEAD, 1), b))
    for k in range(4):
        here = lane // 32 == k
        writes = writes + jnp.where(here, parts[k][:, 128:], 0.0)
        reads = reads + jnp.where(here, parts[4 + k][:, 128:], 0.0)
    gate = jnp.concatenate(gates, axis=1)
    fresh = jnp.concatenate([*values, writes, reads], axis=1)
    ready()
    conv = s["conv"]
    conv_next[0] = conv[1]
    conv_next[1] = conv[2]
    conv_next[2] = fresh.astype(BF16)
    total = fresh * conv_weight[3]
    for t in range(3):
        total = total + conv[t].astype(F32) * conv_weight[t]
    activated = silu(total)
    inputs = activated[:, : PER * HEAD]
    write_vec = activated[:, PER * HEAD : PER * HEAD + STATE]
    read_vec = activated[:, PER * HEAD + STATE :]
    raw_step = parts[3][:, 128 : 128 + PER] + step_bias[...]
    step_size = jnp.maximum(raw_step, 0.0) + jnp.log1p(jnp.exp(-jnp.abs(raw_step)))
    decay = jnp.exp(-step_size * jnp.exp(log_decay_rate[...]))

    def over_heads(v):
        return jnp.concatenate(
            [jnp.where(low, v[:, 2 * j : 2 * j + 1], v[:, 2 * j + 1 : 2 * j + 2]) for j in range(PER // 2)],
            axis=1,
        )

    drive, kept = over_heads(step_size) * inputs, over_heads(decay)
    row = lax.broadcasted_iota(jnp.int32, (ROWS, STATE), 0)
    carried = 0.0
    for b in range(ROWS):
        one = jnp.where(row == b, read_vec, 0.0).astype(BF16)
        flat = state[b].reshape(PER * HEAD, STATE).astype(BF16)
        carried = carried + lax.dot_general(one, flat, (((1,), (1,)), ((), ())), preferred_element_type=F32)
    readout = kept * carried + drive * jnp.sum(write_vec * read_vec, axis=1, keepdims=True)
    gated = readout * silu(gate)
    scale = lax.rsqrt(jnp.mean(gated * gated, axis=1, keepdims=True) + norm_epsilon)
    return (gated * scale * group_gain[...]).astype(BF16), (kept, drive, write_vec)


def update_state(state, kept, drive, write_vec):
    kept, drive = kept.T, drive.T
    for b in range(ROWS):
        flat = state[b].reshape(PER * HEAD, STATE)
        new = flat * kept[:, b : b + 1] + drive[:, b : b + 1] * write_vec[b : b + 1]
        state[b] = new.reshape(PER, HEAD, STATE)


def layer(*refs):
    (stream, gain_1, gain_2, gain_3, step_in, conv_weight, step_bias, log_decay_rate, group_gain) = refs[:9]
    held = dict(zip(STAGED, refs[9 : 9 + len(STAGED)]))
    refs = refs[9 + len(STAGED) :]
    result, conv_next, state_next = refs[:3]
    refs = refs[3:]
    s = dict(zip(SCRATCH, refs))
    sends, recvs, stage_sems, early_sems = refs[len(SCRATCH) :]
    wire = Wire(sends, recvs)
    plain, folded = Plane(wire, False), Plane(wire, True)
    z, x, kv, tp = wire.z, wire.x, wire.kv, wire.tp
    wait_greeting = greet(wire)

    staging = {
        name: pltpu.make_async_copy(held[name], s[name], stage_sems.at[i]) for i, name in enumerate(STAGED)
    }
    for copy in staging.values():
        copy.start()
    a, b = part_of(s, "a_"), part_of(s, "b_")
    staging["a_gate"].wait()
    turn_columns(a["gate"], a["gate_t"])
    staging["a_up"].wait()
    turn_columns(a["up"], a["up_t"])
    wait_greeting()
    sets = {"second": {0: [], 1: []}}

    def second(part, which):
        turned = b["up_t"] if which else b["gate_t"]
        sets["second"][part].append(send_cut(wire, plain, turned, b["both"], part, which))

    def second_down():
        staging["b_down"].wait()
        sets["next_down"] = send_down(wire, plain, b["down"], b["down_parts"])

    early = [
        pltpu.make_async_copy(s["conv_next"], conv_next, early_sems.at[0]),
        pltpu.make_async_copy(s["state"], state_next, early_sems.at[1]),
    ]

    class First(Hooks):
        def after_first_sends(self):
            sets["first"] = {0: [send_cut(wire, plain, a["gate_t"], a["both"], 0, 0)]}
            sets["first"][0].append(send_cut(wire, plain, a["up_t"], a["both"], 0, 1))

        def after_forwards(self):
            sets["first"][1] = [send_cut(wire, plain, a["gate_t"], a["both"], 1, 0)]
            sets["first"][1].append(send_cut(wire, plain, a["up_t"], a["both"], 1, 1))

        def after_sums(self):
            staging["a_down"].wait()
            sets["down"] = send_down(wire, plain, a["down"], a["down_parts"])

        def wait_weights(self, part):
            wait_all(sets["first"][part])

        def after_hidden(self):
            for name in ("gate_in", "value_in", "write_in", "read_in"):
                staging[name].wait()
            turn_mixer(s, step_in)
            for name in ("b_gate", "b_up"):
                staging[name].wait()
            turn_columns(b["gate"], b["gate_t"])
            turn_columns(b["up"], b["up_t"])
            s["mix_in"][:, at_rows(folded.g, FEAT, FEAT)] = s["mix_t"][folded.g]
            wait_down(sets["down"], a["down_parts"], a["down_t"])

        def before_down(self):
            lanes = at_rows(folded.g, FEAT, FEAT)
            sets["mix"] = Copies(wire, s["mix_in"].at[:, 0 : (NZ - 1) * FEAT], True)
            sets["mix"].to_g(folded, lambda peer: s["mix_t"].at[peer], s["mix_in"].at[:, lanes])

    branch = channel_mixer(wire, plain, stream[...], gain_1, a, First(), a["down_t"])
    after = (stream[...].astype(F32) + 0.5 * branch).astype(BF16)

    def early_second():
        second(0, 0)
        second(0, 1)
        second(1, 0)

    squares = gather_features(
        wire, folded, after, gain_2, s["mix_feats"], s["mix_sq_g"], s["mix_sq_tp"], early_second, lambda: None
    )
    wait_all([sets["mix"]])
    part = jnp.dot(s["mix_in"][...], s["mix_feats"][...].reshape(DEPTH, SEQS), preferred_element_type=F32)
    turned = s["turned"]
    turned[2 * HEAD :, :] = jnp.zeros((WIDE - 2 * HEAD, SEQS), F32)
    turned[: 2 * HEAD, :] = part[: 2 * HEAD]
    quarter = lax.rem(folded.g, 4)
    turned[pl.ds(pl.multiple_of(128 + 32 * quarter, 32), 32), :] = part[2 * HEAD : 2 * HEAD + 32]
    beside = pl.multiple_of(128 + 32 * lax.rem(folded.g + 1, 4), 32)
    turned[pl.ds(beside, 8), :] = part[2 * HEAD + 32 : 2 * HEAD + 40]
    turned[pl.ds(pl.multiple_of(beside + 8, 8), 8), :] = jnp.broadcast_to(squares, (8, SEQS))
    rows, rows_in = s["rows"], s["rows_in"]
    rows[...] = turned[...].T.astype(BF16).reshape(NKV, ROWS, WIDE)

    row_copies = Copies(wire, rows.at[0 : NKV - 1])
    offsets = [(dz, dx) for dz in range(NZ) for dx in range(NX) if dz or dx]
    for dz, dx in sorted(offsets, key=lambda o: -min(o[0], NZ - o[0]) - min(o[1], NX - o[1])):
        peer = lax.rem(z + dz, NZ) * NX + lax.rem(x + dx, NX)
        row_copies.send(rows.at[peer], rows_in.at[kv], peer, tp)
    rows_in[kv] = rows[kv]
    wire.settle((row_copies,))
    staging["state"].wait()
    row_copies.arrived(rows_in.at[0 : NKV - 1])
    mixed, change = state_step(
        s,
        folded,
        conv_weight,
        step_bias,
        log_decay_rate,
        group_gain,
        s["conv_next"],
        s["state"],
        lambda: staging["conv"].wait(),
    )

    mixed_all = s["mixed_all"]
    mixed_all[z, x] = mixed
    own = mixed_all.at[z, x]
    to_z = Copies(wire, mixed_all.at[0 : NZ - 1, 0])
    to_x = Copies(wire, mixed_all.at[0 : NZ - 2])
    for d in plain.near:
        to_z.send(own, own, plain.kv_at(plain.ahead(d), x), tp, d)
    to_x.to_h(plain, lambda peer: own, own)
    early[0].start()
    staging["out_weight"].wait()
    wire.settle((to_z, to_x))
    for d in plain.near:
        block = mixed_all.at[plain.behind(d), x]
        to_z.arrived(block, d)
        to_x.to_h(plain, lambda peer: block, block)
    second(1, 1)
    second_down()
    to_x.arrived(to_x.every)
    part = jnp.dot(mixed_all[...].reshape(SEQS, PER * HEAD), s["out_weight"][...], preferred_element_type=F32)
    out_t, out_in = s["out_t"], s["out_in"]
    out_t[...] = part.T.astype(BF16).reshape(NTP, OWN, SEQS)
    to_tp = Copies(wire, out_in.at[0 : NTP - 1])
    to_tp.to_tp(lambda peer: out_t.at[peer], out_in.at[tp])
    out_in[tp] = out_t[tp]
    wire.settle((to_tp,))
    update_state(s["state"], *change)
    early[1].start()
    to_tp.arrived(to_tp.every)
    after = (after.astype(F32) + jnp.sum(out_in[...].astype(F32), axis=0)).astype(BF16)

    assert wire.next[False] == [BULK_LEAVE, BULK_ARRIVE], wire.next

    class Second(Hooks):
        def wait_weights(self, part):
            wait_all(sets["second"][part])

        def after_hidden(self):
            wait_down(sets["next_down"], b["down_parts"], b["down_t"])
            gates_ups = [copies for part in (0, 1) for name in ("first", "second") for copies in sets[name][part]]
            for copies in [sets["down"], sets["mix"], sets["next_down"], *gates_ups]:
                copies.left()
            for copy in early:
                copy.wait()

    wire.start_over()
    branch = channel_mixer(wire, plain, after, gain_3, b, Second(), b["down_t"])
    assert wire.next[True] == [LEAVE, ARRIVE]
    result[...] = (after.astype(F32) + 0.5 * branch).astype(BF16)
    wire.settle()


def finish(*refs):
    far_in, far_out, near = refs[:3], refs[3:6], refs[6:9]
    reads, writes = refs[9:]
    piece = ROWS // PIECES
    pairs = [(far_in[i], near[i], far_out[i]) for i in (0, 1)]
    for i in range(PIECES):
        at = pl.ds(i * piece, piece)
        pairs.append(tuple(ref.at[at] for ref in (far_in[2], near[2], far_out[2])))
    into = [pltpu.make_async_copy(a, b, reads.at[i]) for i, (a, b, _) in enumerate(pairs)]
    out = [pltpu.make_async_copy(b, c, writes.at[i]) for i, (_, b, c) in enumerate(pairs)]
    for copy in into:
        copy.start()
    for first, second in zip(into, out):
        first.wait()
        second.start()
    for copy in out:
        copy.wait()


def on_device(
    stream,
    ssm_state,
    conv_state,
    first_gain,
    first_gate,
    first_up,
    first_down,
    mix_gain,
    gate_in,
    value_in,
    write_in,
    read_in,
    step_in,
    conv_weight,
    step_bias,
    log_decay_rate,
    group_gain,
    out_weight,
    last_norm_gain,
    second_gate,
    second_up,
    second_down,
):
    staged = dict(
        a_gate=first_gate,
        a_up=first_up,
        a_down=first_down,
        gate_in=gate_in,
        value_in=value_in,
        write_in=write_in,
        read_in=read_in,
        b_down=second_down,
        b_gate=second_gate,
        b_up=second_up,
        state=ssm_state,
        conv=conv_state[:, :, 0].transpose(1, 0, 2),
        out_weight=out_weight,
    )
    small = (
        stream.T,
        first_gain[None],
        mix_gain[None],
        last_norm_gain[None],
        step_in.T,
        conv_weight,
        step_bias[None],
        log_decay_rate[None],
        group_gain[None],
    )
    whole = pl.BlockSpec(memory_space=pltpu.VMEM)
    channels = PER * HEAD + 2 * STATE
    channels = PER * HEAD + 2 * STATE
    outs = (
        jax.ShapeDtypeStruct((OWN, SEQS), BF16),
        jax.ShapeDtypeStruct((3, ROWS, channels), BF16),
        jax.ShapeDtypeStruct((ROWS, PER, HEAD, STATE), F32),
    )
    far = pl.BlockSpec(memory_space=pltpu.MemorySpace.HBM)
    parts = pl.pallas_call(
        layer,
        name="layer",
        out_shape=outs,
        in_specs=[whole] * len(small) + [far] * len(STAGED),
        out_specs=[whole] + [far] * (len(outs) - 1),
        scratch_shapes=[pltpu.VMEM(shape, dtype) for shape, dtype in SCRATCH.values()]
        + [
            pltpu.SemaphoreType.DMA((LEAVE,)),
            pltpu.SemaphoreType.DMA((ARRIVE,)),
            pltpu.SemaphoreType.DMA((len(STAGED),)),
            pltpu.SemaphoreType.DMA((len(outs) - 1,)),
        ],
        compiler_params=pltpu.CompilerParams(
            collective_id=0, has_side_effects=True, vmem_limit_bytes=VMEM_LIMIT
        ),
    )(*small, *(staged[name] for name in STAGED))
    result, conv_next, ssm_next = pl.pallas_call(
        finish,
        name="finish",
        out_shape=outs,
        in_specs=[far] * len(outs),
        out_specs=[far] * len(outs),
        scratch_shapes=[pltpu.VMEM(out.shape, out.dtype) for out in outs]
        + [pltpu.SemaphoreType.DMA((PIECES + 2,))] * 2,
        compiler_params=pltpu.CompilerParams(vmem_limit_bytes=VMEM_LIMIT),
    )(*parts)
    return (result.T, ssm_next, conv_next.transpose(1, 0, 2)[:, :, None])


def solution(mesh):
    placed = (
        P(None, ("kv", "tp")),
        P("kv", "tp", None, None),
        P("kv", None, "tp", None),
        P(("kv", "tp")),
        P("kv", "tp"),
        P("kv", "tp"),
        P("tp", "kv"),
        P(("kv", "tp")),
        P("kv", "tp"),
        P("kv", "tp"),
        P("kv", "tp"),
        P("kv", "tp"),
        P("kv", "tp"),
        P(None, "tp", None),
        P("tp"),
        P("tp"),
        P("tp"),
        P("tp", "kv"),
        P(("kv", "tp")),
        P("kv", "tp"),
        P("kv", "tp"),
        P("tp", "kv"),
    )
    return jax.shard_map(
        on_device,
        mesh=mesh,
        in_specs=placed,
        out_specs=(P(None, ("kv", "tp")), P("kv", "tp", None, None), P("kv", None, "tp", None)),
        check_vma=False,
    )
```

```python
import jax
import jax.numpy as jnp
from jax import lax
from jax.experimental import pallas as pl
from jax.experimental.pallas import tpu as pltpu
from jax.sharding import PartitionSpec as P

MESH = pl.DeviceIdType.MESH
F32, BF16 = jnp.float32, jnp.bfloat16

NZ, NX, NY, NC = 8, 4, 4, 2
NKV, NTP = NZ * NX, NY * NC
SEQS, D, FF = 512, 4096, 11264
OWN = D // (NKV * NTP)
FEAT = OWN * NTP
DEPTH = FEAT * NZ
CUT = FF // NTP // NZ
XS = SEQS // NX
ROWS = SEQS // NKV
HEAD, STATE, PER = 64, 128, 8
MIX = 176
WIDE = 256
PARTS = ((0, 96), (96, 80))
norm_epsilon = 1e-06


class Wire:
    def __init__(self, sends, recvs):
        self.sends, self.recvs, self.pending = sends, recvs, []
        self.next = {False: [0, 0], True: [BULK_LEAVE, BULK_ARRIVE]}
        kv, self.tp = lax.axis_index("kv"), lax.axis_index("tp")
        self.kv = kv
        self.z, self.x = lax.div(kv, NX), lax.rem(kv, NX)
        self.y, self.c = lax.div(self.tp, NC), lax.rem(self.tp, NC)
        self.sibling = self.y * NC + (1 - self.c)

    def along_y(self, d):
        return lax.rem(self.y + d, NY)

    def along_tp(self, d):
        return lax.rem(self.tp + d, NTP)

    def start_over(self):
        self.next[False] = [0, 0]

    def take(self, bulk, kind):
        self.next[bulk][kind] += 1
        return self.next[bulk][kind] - 1

    def settle(self, keep=()):
        for copies in self.pending:
            if copies not in keep:
                copies.left()
        self.pending = [copies for copies in self.pending if copies in keep]


class Copies:
    def __init__(self, wire, every, bulk=False):
        self.wire, self.every, self.bulk, self.keys = wire, every, bulk, {}
        self.sem = wire.sends.at[wire.take(bulk, 0)]
        if not bulk:
            wire.pending.append(self)

    def arrival(self, key):
        if key not in self.keys:
            self.keys[key] = self.wire.take(self.bulk, 1)
        return self.wire.recvs.at[self.keys[key]]

    def _copy(self, src, dst, kv, tp, key):
        return pltpu.make_async_remote_copy(
            src_ref=src,
            dst_ref=dst,
            send_sem=self.sem,
            recv_sem=self.arrival(key),
            device_id=(kv, tp),
            device_id_type=MESH,
        )

    def send(self, src, dst, kv, tp, key=0):
        self._copy(src, dst, kv, tp, key).start()

    def arrived(self, whole, key=0):
        self._copy(whole, whole, self.wire.kv, self.wire.sibling, key).wait_recv()

    def left(self):
        self._copy(self.every, self.every, self.wire.kv, self.wire.sibling, next(iter(self.keys))).wait_send()

    def to_y(self, src, dst, key=0):
        wire = self.wire
        for d in (2, 1, 3):
            peer = wire.along_y(d)
            self.send(src(peer), dst, wire.kv, peer * NC + wire.c, key)

    def to_tp(self, src, dst):
        for d in range(1, NTP):
            peer = self.wire.along_tp(d)
            self.send(src(peer), dst, self.wire.kv, peer)

    def to_g(self, plane, src, dst):
        for d in plane.far:
            peer = plane.ahead(d)
            self.send(src(peer), dst, plane.kv_at(peer, plane.h), self.wire.tp)

    def to_h(self, plane, src, dst, key=0):
        for d in (2, 1, 3):
            peer = lax.rem(plane.h + d, NX)
            self.send(src(peer), dst, plane.kv_at(plane.g, peer), self.wire.tp, key)


class Plane:
    def __init__(self, wire, folded):
        self.folded = folded
        if folded:
            self.g, self.h = wire.x + NX * lax.rem(wire.z, 2), lax.div(wire.z, 2)
            self.near = (1, 3, 4, 5, 7, 2, 6)
        else:
            self.g, self.h = wire.z, wire.x
            self.near = (1, 7, 2, 6, 3, 5, 4)
        self.far = self.near[::-1]

    def kv_at(self, g, h):
        if self.folded:
            if isinstance(g, int) and isinstance(h, int):
                return (2 * h + g // NX) * NX + g % NX
            return (2 * h + lax.div(g, NX)) * NX + lax.rem(g, NX)
        return g * NX + h

    def ahead(self, d):
        if not self.folded:
            return lax.rem(self.g + d, NZ)
        x, pair = lax.rem(self.g, NX), lax.div(self.g, NX)
        return lax.rem(x + d % NX, NX) + NX * lax.rem(pair + d // NX, 2)

    def behind(self, d):
        if not self.folded:
            return lax.rem(self.g + NZ - d, NZ)
        x, pair = lax.rem(self.g, NX), lax.div(self.g, NX)
        return lax.rem(x + NX - d % NX, NX) + NX * lax.rem(pair + d // NX, 2)


def greet(wire):
    barrier = pltpu.get_barrier_semaphore()

    def tell(kv, tp):
        pl.semaphore_signal(barrier, inc=1, device_id=(kv, tp), device_id_type=MESH)

    for d in range(1, NZ):
        tell(lax.rem(wire.z + d, NZ) * NX + wire.x, wire.tp)
    for d in range(1, NX):
        x = lax.rem(wire.x + d, NX)
        tell(wire.z * NX + x, wire.tp)
    for d in range(1, NTP):
        tell(wire.kv, wire.along_tp(d))
    return lambda: pl.semaphore_wait(barrier, NZ - 1 + NX - 1 + NTP - 1)


def at_rows(start, size, step):
    return pl.ds(pl.multiple_of(start * step, step), size)


def turn_columns(src, dst):
    for j in range(src.shape[1] // 128):
        dst[j * 128 : (j + 1) * 128, :] = src[:, j * 128 : (j + 1) * 128].T


def send_cut(wire, plane, turned, both, part, second):
    g = plane.g
    lanes = at_rows(g, FEAT, FEAT)
    start, size = PARTS[part]
    at = 2 * start + second * size
    copies = Copies(wire, both.at[at : at + size, 0 : (NZ - 1) * FEAT], True)

    def cut(peer):
        return pl.ds(pl.multiple_of(peer * CUT + start, OWN), size)

    copies.to_g(plane, lambda peer: turned.at[cut(peer), :], both.at[at : at + size, lanes])
    both[at : at + size, lanes] = turned[cut(g), :]
    return copies


class Hooks:
    def after_first_sends(self):
        pass

    def after_forwards(self):
        pass

    def after_sums(self):
        pass

    def wait_weights(self, part):
        pass

    def after_hidden(self):
        pass

    def before_down(self):
        pass


def wait_all(sets):
    for copies in sets:
        copies.arrived(copies.every)


def send_down(wire, plane, down, parts):
    g = plane.g
    copies = Copies(wire, parts.at[0 : NZ - 1], True)
    copies.to_g(plane, lambda peer: down.at[at_rows(peer, CUT, CUT), :], parts.at[g])
    parts[g] = down[at_rows(g, CUT, CUT), :]
    return copies


def wait_down(copies, parts, turned):
    copies.arrived(copies.every)
    for s in range(NZ):
        turned[s] = parts[s].T


def silu(v):
    return v / (1.0 + jnp.exp(-v))


def as_column(row):
    square = jnp.broadcast_to(row, (OWN, OWN))
    same = lax.broadcasted_iota(jnp.int32, (OWN, OWN), 0) == lax.broadcasted_iota(jnp.int32, (OWN, OWN), 1)
    return jnp.sum(jnp.where(same, square, 0.0), axis=1, keepdims=True)


def gather_features(wire, plane, values, gain, feats, sq_g, sq_tp, after_first_sends, after_forwards):
    g, tp, c, sibling = plane.g, wire.tp, wire.c, wire.sibling
    wide = values.astype(F32)
    feats[g, tp] = (wide * as_column(gain[...])).astype(BF16)
    own = feats.at[g, tp]
    to_group = Copies(wire, feats.at[0, 0 : NZ - 1])
    along = Copies(wire, feats.at[0 : NY - 1])
    across = Copies(wire, feats.at[0:NY])

    def hand_on(d, peer):
        block = feats.at[peer, tp]
        along.to_y(lambda p: block, block, d)
        across.send(block, block, wire.kv, sibling)

    hand_on(0, g)
    for d in plane.near:
        to_group.send(own, own, plane.kv_at(plane.ahead(d), plane.h), tp, d)
    sq_g[g] = jnp.sum(wide * wide, axis=0, keepdims=True)
    squares_g = Copies(wire, sq_g.at[0 : NZ - 1])
    squares_g.to_g(plane, lambda peer: sq_g.at[g], sq_g.at[g])
    after_first_sends()
    steps = [(0, g)] + [(d, plane.behind(d)) for d in plane.near]
    for d, peer in steps[1:]:
        to_group.arrived(feats.at[peer, tp], d)
        hand_on(d, peer)
    after_forwards()
    squares_g.arrived(squares_g.every)
    sq_tp[tp] = jnp.sum(sq_g[...], axis=0)
    squares_tp = Copies(wire, sq_tp.at[0 : NTP - 1])
    squares_tp.to_tp(lambda peer: sq_tp.at[tp], sq_tp.at[tp])
    for d, peer in steps:
        along.arrived(feats.at[peer, 0 : NY - 1], d)
        for e in (1, 3, 2):
            block = feats.at[peer, wire.along_y(NY - e) * NC + c]
            across.send(block, block, wire.kv, sibling)
    squares_tp.arrived(squares_tp.every)
    across.arrived(across.every)
    return jnp.sum(sq_tp[...], axis=0)


def channel_mixer(wire, plane, values, gain, s, hooks, down_t):
    g, h = plane.g, plane.h
    squares = gather_features(
        wire, plane, values, gain, s["feats"], s["sq_g"], s["sq_tp"], hooks.after_first_sends, hooks.after_forwards
    )
    sq_h, sums, sums_h, hidden = s["sq_h"], s["sums"], s["sums_h"], s["hidden"]
    sq_h[h] = squares
    squares_h = Copies(wire, sq_h.at[0 : NX - 1])
    squares_h.to_h(plane, lambda peer: sq_h.at[h], sq_h.at[h])
    gathered = list(wire.pending)
    sums_out = []
    for part, (start, size) in enumerate(PARTS):
        hooks.wait_weights(part)
        rows = slice(2 * start, 2 * (start + size))
        sums[rows] = jnp.dot(
            s["both"][rows], s["feats"][...].reshape(DEPTH, SEQS), preferred_element_type=F32
        ).astype(BF16)
        copies = Copies(wire, sums_h.at[0 : NX - 1, rows])
        copies.to_h(plane, lambda peer: sums.at[rows, at_rows(peer, XS, XS)], sums_h.at[h, rows])
        sums_h[h, rows] = sums[rows, at_rows(h, XS, XS)]
        sums_out.append(copies)
    hooks.after_sums()
    squares_h.arrived(squares_h.every)
    s["factor"][...] = lax.rsqrt(jnp.sum(sq_h[...], axis=0) / D + norm_epsilon)
    factor = s["factor"][:, at_rows(h, XS, XS)]
    hidden_out = []
    for (start, size), copies in zip(PARTS, sums_out):
        copies.arrived(copies.every)
        at = 2 * start
        gates = sum(sums_h[p, at : at + size].astype(F32) for p in range(NX)) * factor
        ups = sum(sums_h[p, at + size : at + 2 * size].astype(F32) for p in range(NX)) * factor
        here = hidden.at[start : start + size, at_rows(h, XS, XS)]
        here[...] = (silu(gates) * ups).astype(BF16)
        out = Copies(wire, hidden.at[start : start + size, 0 : SEQS - XS])
        out.to_h(plane, lambda peer: here, here)
        hidden_out.append(out)
    hooks.after_hidden()
    for copies in gathered:
        copies.left()
    wire.pending = [copies for copies in wire.pending if copies not in gathered]
    wait_all(hidden_out)
    hooks.before_down()

    c, y = wire.c, wire.y
    outs, other = s["outs"], s["other"]
    by_y, arrived_y = s["by_y"], s["arrived_y"]
    by_g, arrived_g = s["by_g"], s["arrived_g"]
    order = [(d, plane.ahead(d)) for d in plane.far + (0,)]
    across, along = Copies(wire, other), Copies(wire, by_y.at[0 : NY - 1])
    to_group = Copies(wire, by_g.at[0 : NZ - 1])
    for d, k in order:
        part = jnp.dot(down_t[k], hidden[...], preferred_element_type=F32)
        outs[k] = part.astype(BF16).reshape(NY, NC, OWN, SEQS)
        across.send(outs.at[k, :, 1 - c], other.at[k], wire.kv, wire.sibling, d)
    for d, k in order:
        across.arrived(other.at[k], d)
        by_y[:, k] = (outs[k, :, c].astype(F32) + other[k].astype(F32)).astype(BF16)
        along.to_y(lambda peer: by_y.at[peer, k], arrived_y.at[y, k], d)
        arrived_y[y, k] = by_y[y, k]
    for d, k in order:
        along.arrived(arrived_y.at[0 : NY - 1, k], d)
        by_g[k] = sum(arrived_y[p, k].astype(F32) for p in range(NY)).astype(BF16)
        if d:
            to_group.send(by_g.at[k], arrived_g.at[g], plane.kv_at(k, h), wire.tp)
    arrived_g[g] = by_g[g]
    wire.settle((to_group,))
    to_group.arrived(to_group.every)
    return jnp.sum(arrived_g[...].astype(F32), axis=0)


def ff_scratch(name):
    return {
        name + key: value
        for key, value in dict(
            feats=((NZ, NTP, OWN, SEQS), BF16),
            sq_g=((NZ, 1, SEQS), F32),
            sq_tp=((NTP, 1, SEQS), F32),
            sq_h=((NX, 1, SEQS), F32),
            factor=((1, SEQS), F32),
            gate=((FEAT, NZ * CUT), BF16),
            up=((FEAT, NZ * CUT), BF16),
            down=((NZ * CUT, FEAT), BF16),
            gate_t=((NZ * CUT, FEAT), BF16),
            up_t=((NZ * CUT, FEAT), BF16),
            both=((2 * CUT, DEPTH), BF16),
            down_parts=((NZ, CUT, FEAT), BF16),
            down_t=((NZ, FEAT, CUT), BF16),
            sums=((2 * CUT, SEQS), BF16),
            sums_h=((NX, 2 * CUT, XS), BF16),
            hidden=((CUT, SEQS), BF16),
            outs=((NZ, NY, NC, OWN, SEQS), BF16),
            other=((NZ, NY, OWN, SEQS), BF16),
            by_y=((NY, NZ, OWN, SEQS), BF16),
            arrived_y=((NY, NZ, OWN, SEQS), BF16),
            by_g=((NZ, OWN, SEQS), BF16),
            arrived_g=((NZ, OWN, SEQS), BF16),
        ).items()
    }


SCRATCH = dict(
    ff_scratch("a_"),
    **ff_scratch("b_"),
    gate_in=((FEAT, PER * HEAD), BF16),
    value_in=((FEAT, PER * HEAD), BF16),
    write_in=((FEAT, STATE), BF16),
    read_in=((FEAT, STATE), BF16),
    out_weight=((PER * HEAD, FEAT), BF16),
    state=((ROWS, PER, HEAD, STATE), F32),
    conv=((3, ROWS, PER * HEAD + 2 * STATE), BF16),
    conv_next=((3, ROWS, PER * HEAD + 2 * STATE), BF16),
    mix_t=((NZ, MIX, FEAT), BF16),
    mix_in=((MIX, DEPTH), BF16),
    mix_feats=((NZ, NTP, OWN, SEQS), BF16),
    mix_sq_g=((NZ, 1, SEQS), F32),
    mix_sq_tp=((NTP, 1, SEQS), F32),
    turned=((WIDE, SEQS), F32),
    rows=((NKV, ROWS, WIDE), BF16),
    rows_in=((NKV, ROWS, WIDE), BF16),
    mixed_all=((NZ, NX, ROWS, PER * HEAD), BF16),
    out_t=((NTP, OWN, SEQS), BF16),
    out_in=((NTP, OWN, SEQS), BF16),
)
STAGED = (
    "a_gate",
    "a_up",
    "a_down",
    "gate_in",
    "value_in",
    "write_in",
    "read_in",
    "b_down",
    "b_gate",
    "b_up",
    "state",
    "conv",
    "out_weight",
)
BULK_LEAVE, BULK_ARRIVE = 22, 68
LEAVE, ARRIVE = BULK_LEAVE + 11, BULK_ARRIVE + 11
PIECES = 4
VMEM_LIMIT = 58 * 1024 * 1024


def part_of(scratch, name):
    return {key[len(name) :]: ref for key, ref in scratch.items() if key.startswith(name)}


def turn_mixer(s, step_in):
    mix_t = s["mix_t"]
    for j in range(PER * HEAD // 128):
        for ref, at in ((s["gate_in"], 0), (s["value_in"], HEAD)):
            tile = ref[:, j * 128 : (j + 1) * 128].T
            mix_t[2 * j, at : at + HEAD] = tile[:HEAD]
            mix_t[2 * j + 1, at : at + HEAD] = tile[HEAD:]
    for ref, base in ((s["write_in"], 0), (s["read_in"], 4)):
        tile = ref[...].T
        for j in range(4):
            mix_t[base + j, 2 * HEAD : 2 * HEAD + 32] = tile[32 * j : 32 * (j + 1)]
    steps = jnp.concatenate([step_in[...].astype(F32), jnp.zeros((8, FEAT), F32)], axis=0).astype(BF16)
    for j in range(NZ):
        mix_t[j, 2 * HEAD + 32 : MIX] = steps


def state_step(s, plane, conv_weight, step_bias, log_decay_rate, group_gain, conv_next, state, ready):
    rows_in = s["rows_in"]
    parts = [sum(rows_in[plane.kv_at(k, p)].astype(F32) for p in range(NX)) for k in range(NZ)]
    factor = lax.rsqrt(parts[3][:, 2 * HEAD + 8 : 2 * HEAD + 9] / D + norm_epsilon)
    parts = [(part * factor).astype(BF16).astype(F32) for part in parts]
    lane = lax.broadcasted_iota(jnp.int32, (ROWS, 128), 1)
    low = lane < HEAD
    gates, values, writes, reads = [], [], 0.0, 0.0
    for j in range(PER // 2):
        a, b = parts[2 * j][:, :128], parts[2 * j + 1][:, :128]
        gates.append(jnp.where(low, a, pltpu.roll(b, HEAD, 1)))
        values.append(jnp.where(low, pltpu.roll(a, HEAD, 1), b))
    for k in range(4):
        here = lane // 32 == k
        writes = writes + jnp.where(here, parts[k][:, 128:], 0.0)
        reads = reads + jnp.where(here, parts[4 + k][:, 128:], 0.0)
    gate = jnp.concatenate(gates, axis=1)
    fresh = jnp.concatenate([*values, writes, reads], axis=1)
    ready()
    conv = s["conv"]
    conv_next[0] = conv[1]
    conv_next[1] = conv[2]
    conv_next[2] = fresh.astype(BF16)
    total = fresh * conv_weight[3]
    for t in range(3):
        total = total + conv[t].astype(F32) * conv_weight[t]
    activated = silu(total)
    inputs = activated[:, : PER * HEAD]
    write_vec = activated[:, PER * HEAD : PER * HEAD + STATE]
    read_vec = activated[:, PER * HEAD + STATE :]
    raw_step = parts[3][:, 128 : 128 + PER] + step_bias[...]
    step_size = jnp.maximum(raw_step, 0.0) + jnp.log1p(jnp.exp(-jnp.abs(raw_step)))
    decay = jnp.exp(-step_size * jnp.exp(log_decay_rate[...]))

    def over_heads(v):
        return jnp.concatenate(
            [jnp.where(low, v[:, 2 * j : 2 * j + 1], v[:, 2 * j + 1 : 2 * j + 2]) for j in range(PER // 2)],
            axis=1,
        )

    drive, kept = over_heads(step_size) * inputs, over_heads(decay)
    row = lax.broadcasted_iota(jnp.int32, (ROWS, STATE), 0)
    carried = 0.0
    for b in range(ROWS):
        one = jnp.where(row == b, read_vec, 0.0).astype(BF16)
        flat = state[b].reshape(PER * HEAD, STATE).astype(BF16)
        carried = carried + lax.dot_general(one, flat, (((1,), (1,)), ((), ())), preferred_element_type=F32)
    readout = kept * carried + drive * jnp.sum(write_vec * read_vec, axis=1, keepdims=True)
    gated = readout * silu(gate)
    scale = lax.rsqrt(jnp.mean(gated * gated, axis=1, keepdims=True) + norm_epsilon)
    return (gated * scale * group_gain[...]).astype(BF16), (kept, drive, write_vec)


def update_state(state, kept, drive, write_vec):
    kept, drive = kept.T, drive.T
    for b in range(ROWS):
        flat = state[b].reshape(PER * HEAD, STATE)
        new = flat * kept[:, b : b + 1] + drive[:, b : b + 1] * write_vec[b : b + 1]
        state[b] = new.reshape(PER, HEAD, STATE)


def layer(*refs):
    (stream, gain_1, gain_2, gain_3, step_in, conv_weight, step_bias, log_decay_rate, group_gain) = refs[:9]
    held = dict(zip(STAGED, refs[9 : 9 + len(STAGED)]))
    refs = refs[9 + len(STAGED) :]
    result, conv_next, state_next = refs[:3]
    refs = refs[3:]
    s = dict(zip(SCRATCH, refs))
    sends, recvs, stage_sems, early_sems = refs[len(SCRATCH) :]
    wire = Wire(sends, recvs)
    plain, folded = Plane(wire, False), Plane(wire, True)
    z, x, kv, tp = wire.z, wire.x, wire.kv, wire.tp
    wait_greeting = greet(wire)

    staging = {
        name: pltpu.make_async_copy(held[name], s[name], stage_sems.at[i]) for i, name in enumerate(STAGED)
    }
    for copy in staging.values():
        copy.start()
    a, b = part_of(s, "a_"), part_of(s, "b_")
    staging["a_gate"].wait()
    turn_columns(a["gate"], a["gate_t"])
    staging["a_up"].wait()
    turn_columns(a["up"], a["up_t"])
    wait_greeting()
    sets = {"second": {0: [], 1: []}}

    def second(part, which):
        turned = b["up_t"] if which else b["gate_t"]
        sets["second"][part].append(send_cut(wire, plain, turned, b["both"], part, which))

    def second_down():
        staging["b_down"].wait()
        sets["next_down"] = send_down(wire, plain, b["down"], b["down_parts"])

    early = [
        pltpu.make_async_copy(s["conv_next"], conv_next, early_sems.at[0]),
        pltpu.make_async_copy(s["state"], state_next, early_sems.at[1]),
    ]

    class First(Hooks):
        def after_first_sends(self):
            sets["first"] = {0: [send_cut(wire, plain, a["gate_t"], a["both"], 0, 0)]}
            sets["first"][0].append(send_cut(wire, plain, a["up_t"], a["both"], 0, 1))

        def after_forwards(self):
            sets["first"][1] = [send_cut(wire, plain, a["gate_t"], a["both"], 1, 0)]
            sets["first"][1].append(send_cut(wire, plain, a["up_t"], a["both"], 1, 1))

        def after_sums(self):
            staging["a_down"].wait()
            sets["down"] = send_down(wire, plain, a["down"], a["down_parts"])

        def wait_weights(self, part):
            if part == 0:
                for name in ("b_gate", "b_up"):
                    staging[name].wait()
                turn_columns(b["gate"], b["gate_t"])
                turn_columns(b["up"], b["up_t"])
            wait_all(sets["first"][part])

        def after_hidden(self):
            for name in ("gate_in", "value_in", "write_in", "read_in"):
                staging[name].wait()
            turn_mixer(s, step_in)
            s["mix_in"][:, at_rows(folded.g, FEAT, FEAT)] = s["mix_t"][folded.g]
            wait_down(sets["down"], a["down_parts"], a["down_t"])

        def before_down(self):
            lanes = at_rows(folded.g, FEAT, FEAT)
            sets["mix"] = Copies(wire, s["mix_in"].at[:, 0 : (NZ - 1) * FEAT], True)
            sets["mix"].to_g(folded, lambda peer: s["mix_t"].at[peer], s["mix_in"].at[:, lanes])

    branch = channel_mixer(wire, plain, stream[...], gain_1, a, First(), a["down_t"])
    after = (stream[...].astype(F32) + 0.5 * branch).astype(BF16)

    def early_second():
        second(0, 0)
        second(0, 1)
        second(1, 0)

    squares = gather_features(
        wire, folded, after, gain_2, s["mix_feats"], s["mix_sq_g"], s["mix_sq_tp"], early_second, lambda: None
    )
    wait_all([sets["mix"]])
    part = jnp.dot(s["mix_in"][...], s["mix_feats"][...].reshape(DEPTH, SEQS), preferred_element_type=F32)
    turned = s["turned"]
    turned[2 * HEAD :, :] = jnp.zeros((WIDE - 2 * HEAD, SEQS), F32)
    turned[: 2 * HEAD, :] = part[: 2 * HEAD]
    quarter = lax.rem(folded.g, 4)
    turned[pl.ds(pl.multiple_of(128 + 32 * quarter, 32), 32), :] = part[2 * HEAD : 2 * HEAD + 32]
    beside = pl.multiple_of(128 + 32 * lax.rem(folded.g + 1, 4), 32)
    turned[pl.ds(beside, 8), :] = part[2 * HEAD + 32 : 2 * HEAD + 40]
    turned[pl.ds(pl.multiple_of(beside + 8, 8), 8), :] = jnp.broadcast_to(squares, (8, SEQS))
    rows, rows_in = s["rows"], s["rows_in"]
    rows[...] = turned[...].T.astype(BF16).reshape(NKV, ROWS, WIDE)

    row_copies = Copies(wire, rows.at[0 : NKV - 1])
    offsets = [(dz, dx) for dz in range(NZ) for dx in range(NX) if dz or dx]
    for dz, dx in sorted(offsets, key=lambda o: -min(o[0], NZ - o[0]) - min(o[1], NX - o[1])):
        peer = lax.rem(z + dz, NZ) * NX + lax.rem(x + dx, NX)
        row_copies.send(rows.at[peer], rows_in.at[kv], peer, tp)
    rows_in[kv] = rows[kv]
    wire.settle((row_copies,))
    staging["state"].wait()
    row_copies.arrived(rows_in.at[0 : NKV - 1])
    mixed, change = state_step(
        s,
        folded,
        conv_weight,
        step_bias,
        log_decay_rate,
        group_gain,
        s["conv_next"],
        s["state"],
        lambda: staging["conv"].wait(),
    )

    mixed_all = s["mixed_all"]
    mixed_all[z, x] = mixed
    own = mixed_all.at[z, x]
    to_z = Copies(wire, mixed_all.at[0 : NZ - 1, 0])
    to_x = Copies(wire, mixed_all.at[0 : NZ - 2])
    for d in plain.near:
        to_z.send(own, own, plain.kv_at(plain.ahead(d), x), tp, d)
    to_x.to_h(plain, lambda peer: own, own)
    early[0].start()
    staging["out_weight"].wait()
    wire.settle((to_z, to_x))
    for d in plain.near:
        block = mixed_all.at[plain.behind(d), x]
        to_z.arrived(block, d)
        to_x.to_h(plain, lambda peer: block, block)
    second(1, 1)
    second_down()
    to_x.arrived(to_x.every)
    part = jnp.dot(mixed_all[...].reshape(SEQS, PER * HEAD), s["out_weight"][...], preferred_element_type=F32)
    out_t, out_in = s["out_t"], s["out_in"]
    out_t[...] = part.T.astype(BF16).reshape(NTP, OWN, SEQS)
    to_tp = Copies(wire, out_in.at[0 : NTP - 1])
    to_tp.to_tp(lambda peer: out_t.at[peer], out_in.at[tp])
    out_in[tp] = out_t[tp]
    wire.settle((to_tp,))
    update_state(s["state"], *change)
    early[1].start()
    to_tp.arrived(to_tp.every)
    after = (after.astype(F32) + jnp.sum(out_in[...].astype(F32), axis=0)).astype(BF16)

    assert wire.next[False] == [BULK_LEAVE, BULK_ARRIVE], wire.next

    class Second(Hooks):
        def wait_weights(self, part):
            wait_all(sets["second"][part])

        def after_hidden(self):
            wait_down(sets["next_down"], b["down_parts"], b["down_t"])
            gates_ups = [copies for part in (0, 1) for name in ("first", "second") for copies in sets[name][part]]
            for copies in [sets["down"], sets["mix"], sets["next_down"], *gates_ups]:
                copies.left()
            for copy in early:
                copy.wait()

    wire.start_over()
    branch = channel_mixer(wire, plain, after, gain_3, b, Second(), b["down_t"])
    assert wire.next[True] == [LEAVE, ARRIVE]
    result[...] = (after.astype(F32) + 0.5 * branch).astype(BF16)
    wire.settle()


def finish(*refs):
    far_in, far_out, near = refs[:3], refs[3:6], refs[6:9]
    reads, writes = refs[9:]
    piece = ROWS // PIECES
    pairs = [(far_in[i], near[i], far_out[i]) for i in (0, 1)]
    for i in range(PIECES):
        at = pl.ds(i * piece, piece)
        pairs.append(tuple(ref.at[at] for ref in (far_in[2], near[2], far_out[2])))
    into = [pltpu.make_async_copy(a, b, reads.at[i]) for i, (a, b, _) in enumerate(pairs)]
    out = [pltpu.make_async_copy(b, c, writes.at[i]) for i, (_, b, c) in enumerate(pairs)]
    for copy in into:
        copy.start()
    for first, second in zip(into, out):
        first.wait()
        second.start()
    for copy in out:
        copy.wait()


def on_device(
    stream,
    ssm_state,
    conv_state,
    first_gain,
    first_gate,
    first_up,
    first_down,
    mix_gain,
    gate_in,
    value_in,
    write_in,
    read_in,
    step_in,
    conv_weight,
    step_bias,
    log_decay_rate,
    group_gain,
    out_weight,
    last_norm_gain,
    second_gate,
    second_up,
    second_down,
):
    staged = dict(
        a_gate=first_gate,
        a_up=first_up,
        a_down=first_down,
        gate_in=gate_in,
        value_in=value_in,
        write_in=write_in,
        read_in=read_in,
        b_down=second_down,
        b_gate=second_gate,
        b_up=second_up,
        state=ssm_state,
        conv=conv_state[:, :, 0].transpose(1, 0, 2),
        out_weight=out_weight,
    )
    small = (
        stream.T,
        first_gain[None],
        mix_gain[None],
        last_norm_gain[None],
        step_in.T,
        conv_weight,
        step_bias[None],
        log_decay_rate[None],
        group_gain[None],
    )
    whole = pl.BlockSpec(memory_space=pltpu.VMEM)
    channels = PER * HEAD + 2 * STATE
    channels = PER * HEAD + 2 * STATE
    outs = (
        jax.ShapeDtypeStruct((OWN, SEQS), BF16),
        jax.ShapeDtypeStruct((3, ROWS, channels), BF16),
        jax.ShapeDtypeStruct((ROWS, PER, HEAD, STATE), F32),
    )
    far = pl.BlockSpec(memory_space=pltpu.MemorySpace.HBM)
    parts = pl.pallas_call(
        layer,
        name="layer",
        out_shape=outs,
        in_specs=[whole] * len(small) + [far] * len(STAGED),
        out_specs=[whole] + [far] * (len(outs) - 1),
        scratch_shapes=[pltpu.VMEM(shape, dtype) for shape, dtype in SCRATCH.values()]
        + [
            pltpu.SemaphoreType.DMA((LEAVE,)),
            pltpu.SemaphoreType.DMA((ARRIVE,)),
            pltpu.SemaphoreType.DMA((len(STAGED),)),
            pltpu.SemaphoreType.DMA((len(outs) - 1,)),
        ],
        compiler_params=pltpu.CompilerParams(
            collective_id=0, has_side_effects=True, vmem_limit_bytes=VMEM_LIMIT
        ),
    )(*small, *(staged[name] for name in STAGED))
    result, conv_next, ssm_next = pl.pallas_call(
        finish,
        name="finish",
        out_shape=outs,
        in_specs=[far] * len(outs),
        out_specs=[far] * len(outs),
        scratch_shapes=[pltpu.VMEM(out.shape, out.dtype) for out in outs]
        + [pltpu.SemaphoreType.DMA((PIECES + 2,))] * 2,
        compiler_params=pltpu.CompilerParams(vmem_limit_bytes=VMEM_LIMIT),
    )(*parts)
    return (result.T, ssm_next, conv_next.transpose(1, 0, 2)[:, :, None])


def solution(mesh):
    placed = (
        P(None, ("kv", "tp")),
        P("kv", "tp", None, None),
        P("kv", None, "tp", None),
        P(("kv", "tp")),
        P("kv", "tp"),
        P("kv", "tp"),
        P("tp", "kv"),
        P(("kv", "tp")),
        P("kv", "tp"),
        P("kv", "tp"),
        P("kv", "tp"),
        P("kv", "tp"),
        P("kv", "tp"),
        P(None, "tp", None),
        P("tp"),
        P("tp"),
        P("tp"),
        P("tp", "kv"),
        P(("kv", "tp")),
        P("kv", "tp"),
        P("kv", "tp"),
        P("tp", "kv"),
    )
    return jax.shard_map(
        on_device,
        mesh=mesh,
        in_specs=placed,
        out_specs=(P(None, ("kv", "tp")), P("kv", "tp", None, None), P("kv", None, "tp", None)),
        check_vma=False,
    )
```
